512 devices in a mesh: sp: 64 (over z, y), tp: 8 (over x, core).
Axes of the slice: x: 4, y: 8, z: 8, core: 2. Of those that a mesh axis runs over, the one named last changes fastest.
Arguments:
- tokens: bfloat16 [14336, 2048], P('sp', 'tp'), may hold values from -6 to 6
- norm_gain: float32 [2048], replicated, may hold values from 0.1 to 1.9
- query_weight: bfloat16 [2048, 2048], P('sp', 'tp'), may hold values from -0.125 to 0.125
- key_weight: bfloat16 [2048, 1024], P('sp', 'tp'), may hold values from -0.125 to 0.125
- value_weight: bfloat16 [2048, 1024], P('sp', 'tp'), may hold values from -0.125 to 0.125
- glu_value_weight: bfloat16 [2048, 1536], P('sp', 'tp'), may hold values from -0.125 to 0.125
- glu_gate_weight: bfloat16 [2048, 1536], P('sp', 'tp'), may hold values from -0.125 to 0.125
- query_gain: float32 [64], replicated, may hold values from 1.2 to 1.6
- key_gain: float32 [64], replicated, may hold values from 1.1 to 1.4
- lambdas: float32 [16], P('tp'), may hold values from 0.3 to 0.8
- head_gain: float32 [128], replicated, may hold values from 0.1 to 1.9
- conv_weight: float32 [31, 1536], P(None, 'tp'), may hold values from -11 to 11
- channel_gain: float32 [1536], P('tp'), may hold values from 0.1 to 1.9
- attn_out_weight: bfloat16 [2048, 2048], P('sp', 'tp'), may hold values from -0.09375 to 0.09375
- conv_out_weight: bfloat16 [2048, 1536], P('sp', 'tp'), may hold values from -0.09375 to 0.09375
Outputs:
- mixed: bfloat16 [14336, 2048], P(('sp', 'tp'))
The draws below stay inside these ranges and needn't reach their ends.
All inputs are finite; a program needn't handle non-finite values.
Results may differ from the reference program's by a relative error of at most 0.014.
Values may be sent and summed in bfloat16 or wider, within the bound.
No kernel may reach another device: no remote copies, remote signals or barrier semaphores. Data moves between devices by JAX's collectives and lax.ppermute only.
A program may use at most 64 MiB of HBM per device.

```python
import math
import jax
import jax.numpy as jnp
from jax import lax

D = 2048
HEADS = 16
KV_HEADS = 8
HEAD_DIM = 64
C_CH = 1536
CONV_W = 31
TOK_DEV = 224
SEQ = 14336


def draw_conv_weight(key, part):
    column = jnp.arange(C_CH, dtype=jnp.float32) / max(C_CH - 1, 1)
    base = jax.random.truncated_normal(key, -6.0, 6.0, (CONV_W, C_CH), jnp.float32)
    spread = jnp.exp(column * math.log(10.0))
    return base * spread * CONV_W ** (-0.5)


def shard_levels(key, extent, pieces, low, high):
    def one(position, blocks):
        draws = jax.random.uniform(jax.random.fold_in(jax.random.fold_in(key, 6), position), (blocks,), jnp.float32, low / len(pieces), high / len(pieces))
        return jnp.repeat(jnp.exp(draws), extent[position] // blocks).reshape((-1,) + (1,) * (len(extent) - position - 1))

    factor_of = one(*pieces[0])
    for cut in pieces[1:]:
        factor_of = factor_of * one(*cut)
    return factor_of


def centred(rng, shape, deviation, limit, cuts=(), held_as=jnp.bfloat16):
    drawn = jax.random.normal(rng, shape, jnp.float32) * deviation
    if len(cuts) > 0:
        drawn = shard_levels(rng, shape, cuts, -0.22, 0.18) * drawn
    return jnp.clip(drawn, min=-limit, max=limit).astype(held_as)


def setup_inputs(seed: int = 0) -> dict:
    splits = jax.random.split(jax.random.key(seed), 16)
    tokens = centred(splits[0], (SEQ, D), 1.0, 6.0, ((0, 64), (1, 8)))
    norm_gain = jnp.clip(1.0 + 0.18 * jax.random.normal(splits[1], (D,), jnp.float32), 0.1, 1.9)
    query_weight = centred(splits[2], (D, 2 * HEADS * HEAD_DIM), D ** -0.5, 0.125, ((0, 64), (1, 8)))
    key_weight = centred(splits[3], (D, 2 * KV_HEADS * HEAD_DIM), D ** -0.5, 0.125, ((0, 64), (1, 8)))
    value_weight = centred(splits[4], (D, 2 * KV_HEADS * HEAD_DIM), D ** -0.5, 0.125, ((0, 64), (1, 8)))
    glu_value_weight = centred(splits[5], (D, C_CH), D ** -0.5, 0.125, ((0, 64), (1, 8)))
    glu_gate_weight = centred(splits[6], (D, C_CH), D ** -0.5, 0.125, ((0, 64), (1, 8)))
    query_gain = jnp.clip(jax.random.uniform(splits[7], (HEAD_DIM,), jnp.float32, 1.2, 1.6), 1.2, 1.6)
    key_gain = jnp.clip(jax.random.uniform(splits[8], (HEAD_DIM,), jnp.float32, 1.1, 1.4), 1.1, 1.4)
    lambdas = jnp.clip(0.3 + 0.5 * jax.random.uniform(splits[9], (HEADS,), jnp.float32) ** shard_levels(splits[9], (HEADS,), ((0, 8),), -0.2, 0.2), 0.3, 0.8)
    head_gain = jnp.clip(1.0 + 0.18 * jax.random.normal(splits[10], (2 * HEAD_DIM,), jnp.float32), 0.1, 1.9)
    conv_weight = draw_conv_weight(jax.random.fold_in(splits[15], 71), 0)
    channel_gain = jnp.clip(1.0 + 0.18 * jax.random.normal(splits[12], (C_CH,), jnp.float32), 0.1, 1.9)
    attn_out_weight = centred(splits[13], (D, 2 * HEADS * HEAD_DIM), (2 * HEADS * HEAD_DIM + C_CH) ** -0.5, 0.09375, ((0, 64), (1, 8)))
    conv_out_weight = centred(splits[14], (D, C_CH), (2 * HEADS * HEAD_DIM + C_CH) ** -0.5, 0.09375, ((0, 64), (1, 8)))
    return {"tokens": tokens, "norm_gain": norm_gain, "query_weight": query_weight, "key_weight": key_weight, "value_weight": value_weight, "glu_value_weight": glu_value_weight, "glu_gate_weight": glu_gate_weight, "query_gain": query_gain, "key_gain": key_gain, "lambdas": lambdas, "head_gain": head_gain, "conv_weight": conv_weight, "channel_gain": channel_gain, "attn_out_weight": attn_out_weight, "conv_out_weight": conv_out_weight}


EPS = 1e-06
LAMBDA_INIT = 0.2

def rms_scale(values, gain):
    return values * lax.rsqrt(lax.optimization_barrier(jnp.mean(values * values, axis=-1, keepdims=True)) + EPS) * gain

def reference(tokens, norm_gain, query_weight, key_weight, value_weight, glu_value_weight, glu_gate_weight, query_gain, key_gain, lambdas, head_gain, conv_weight, channel_gain, attn_out_weight, conv_out_weight):
    seq_len = tokens.shape[0]
    normed = rms_scale(tokens.astype(jnp.float32), norm_gain).astype(jnp.bfloat16)
    queries = jnp.dot(normed, query_weight, preferred_element_type=jnp.float32).reshape(seq_len, HEADS, 2, HEAD_DIM)
    query_normed = rms_scale(queries, query_gain).astype(jnp.bfloat16)
    keys = jnp.dot(normed, key_weight, preferred_element_type=jnp.float32).reshape(seq_len, KV_HEADS, 2, HEAD_DIM)
    key_normed = rms_scale(keys, key_gain).astype(jnp.bfloat16)
    values = jnp.dot(normed, value_weight, preferred_element_type=jnp.float32).astype(jnp.bfloat16)
    values = values.reshape(seq_len, KV_HEADS, 2 * HEAD_DIM)
    group = HEADS // KV_HEADS
    key_all = jnp.repeat(key_normed, group, axis=1)
    value_all = jnp.repeat(values, group, axis=1)

    def one_head(inputs):
        head_query, head_key, head_value, weight_two = inputs
        key_float = head_key.astype(jnp.float32)
        value_float = head_value.astype(jnp.float32)

        def one_block(block_query):
            scores = jnp.einsum('bpd,npd->pbn', block_query.astype(jnp.float32), key_float) * HEAD_DIM ** (-0.5)
            expo = jnp.exp(scores - lax.optimization_barrier(jnp.max(scores, axis=-1, keepdims=True)))
            totals = lax.optimization_barrier(jnp.sum(expo, axis=-1))
            rounded = lax.optimization_barrier(expo.astype(jnp.bfloat16)).astype(jnp.float32)
            numer = jnp.einsum('pbn,nd->pbd', rounded, value_float)
            ratio = numer / totals[..., None]
            return ratio[0] - weight_two * ratio[1]
        blocks = lax.map(one_block, head_query.reshape(seq_len // TOK_DEV, TOK_DEV, 2, HEAD_DIM))
        return blocks.reshape(seq_len, 2 * HEAD_DIM)
    head_outs = lax.map(one_head, (query_normed.transpose(1, 0, 2, 3), key_all.transpose(1, 0, 2, 3), value_all.transpose(1, 0, 2), lambdas))
    att_rows = head_outs.transpose(1, 0, 2)
    att_out = (rms_scale(att_rows, head_gain) * (1.0 - LAMBDA_INIT)).astype(jnp.bfloat16)
    att_out = att_out.reshape(seq_len, HEADS * 2 * HEAD_DIM)
    glu_value = jnp.dot(normed, glu_value_weight, preferred_element_type=jnp.float32)
    glu_gate = jnp.dot(normed, glu_gate_weight, preferred_element_type=jnp.float32)
    glu_rows = (glu_value * jax.nn.sigmoid(glu_gate)).astype(jnp.bfloat16)
    reach = CONV_W // 2
    padded = jnp.pad(glu_rows.astype(jnp.float32), ((reach, reach), (0, 0)))
    conv_sum = jnp.zeros((seq_len, C_CH), jnp.float32)
    for offset in range(CONV_W):
        conv_sum = conv_sum + conv_weight[offset] * padded[offset:offset + seq_len]
    conv_out = jax.nn.silu(rms_scale(conv_sum, channel_gain)).astype(jnp.bfloat16)
    term = jnp.dot(att_out, attn_out_weight.T, preferred_element_type=jnp.float32)
    term = term + jnp.dot(conv_out, conv_out_weight.T, preferred_element_type=jnp.float32)
    return term.astype(jnp.bfloat16)
```

```python
import functools
import math

import jax
import jax.numpy as jnp
from jax import lax
from jax.experimental import pallas as pl
from jax.experimental.pallas import tpu as pltpu
from jax.sharding import Mesh
from jax.sharding import PartitionSpec as P

HEAD_DIM = 64
C_CH = 1536
CONV_W = 31
TP = ("x", "c")
SP_TP = ("sp", "x", "c")
EPS = 1e-06
LAMBDA_INIT = 0.2
BF = jnp.bfloat16
F32 = jnp.float32


def rms_scale(values, gain):
    return values * lax.rsqrt(jnp.mean(values * values, axis=-1, keepdims=True) + EPS) * gain


def contract_last(left, right):
    return lax.dot_general(left, right, (((1,), (1,)), ((), ())), preferred_element_type=F32)


def attend_kernel(q_ref, k_ref, v_ref, o_ref, *, rows, keys):
    @pl.when(pl.program_id(0) == 0)
    def _():
        o_ref[...] = jnp.zeros_like(o_ref)

    ones = jnp.ones((keys, 2 * HEAD_DIM), BF)
    for j in range(k_ref.shape[0] // keys):
        k = k_ref[j * keys : (j + 1) * keys, :]
        v = jnp.concatenate([v_ref[j * keys : (j + 1) * keys, :], ones], axis=1)
        for r in range(q_ref.shape[0] // rows):
            part = pl.ds(r * rows, rows)
            s = contract_last(q_ref[part, :], k)
            e = jnp.exp2(s).astype(BF)
            o_ref[part, :] += jnp.dot(e, v, preferred_element_type=F32)


def attend(q_rows, kv, block, rows, keys):
    count, total = q_rows.shape[0], kv.shape[0]
    width = 2 * HEAD_DIM
    return pl.pallas_call(
        functools.partial(attend_kernel, rows=rows, keys=keys),
        grid=(total // block,),
        in_specs=[
            pl.BlockSpec((count, width), lambda i: (0, 0)),
            pl.BlockSpec((block, width), lambda i: (i, 0)),
            pl.BlockSpec((block, width), lambda i: (i, 1)),
        ],
        out_specs=pl.BlockSpec((count, 2 * width), lambda i: (0, 0)),
        out_shape=jax.ShapeDtypeStruct((count, 2 * width), F32),
        cost_estimate=pl.CostEstimate(
            flops=6 * count * total * width,
            transcendentals=count * total,
            bytes_accessed=total * 4 * width + count * 10 * width,
        ),
        name="attend",
    )(q_rows, kv, kv)


def local(
    tokens,
    norm_gain,
    query_weight,
    key_weight,
    value_weight,
    glu_value_weight,
    glu_gate_weight,
    query_gain,
    key_gain,
    lambdas,
    head_gain,
    conv_weight,
    channel_gain,
    attn_out_weight,
    conv_out_weight,
):
    weights = (
        query_weight,
        key_weight,
        value_weight,
        glu_value_weight,
        glu_gate_weight,
        attn_out_weight,
        conv_out_weight,
    )
    ends = [0]
    for w in weights:
        ends.append(ends[-1] + w.shape[1])
    gathered_w = lax.all_gather(jnp.concatenate(weights, axis=1), "sp", axis=0, tiled=True)
    wq, wk, wv, wgv, wgg, wao, wco = (
        gathered_w[:, ends[i] : ends[i + 1]] for i in range(len(weights))
    )

    gathered = lax.all_gather(tokens, TP, axis=1, tiled=True).astype(F32)
    normed = rms_scale(gathered, norm_gain).astype(BF)
    tok_rows = normed.shape[0]

    def project(w):
        return jnp.dot(normed, w, preferred_element_type=F32)

    q_heads = query_weight.shape[1] // (2 * HEAD_DIM)
    kv_heads = key_weight.shape[1] // (2 * HEAD_DIM)
    width = 2 * HEAD_DIM
    key_rows = rms_scale(project(wk).reshape(tok_rows, 2 * kv_heads, HEAD_DIM), key_gain)
    kv_rows = jnp.concatenate(
        [key_rows.astype(BF).reshape(tok_rows, width * kv_heads), project(wv).astype(BF)], axis=1
    )
    kv = lax.all_gather(kv_rows, "sp", axis=0, tiled=True)

    fold = math.log2(math.e) * HEAD_DIM ** (-0.5)
    queries = project(wq).reshape(tok_rows, 2 * q_heads, HEAD_DIM)
    q_normed = rms_scale(queries, query_gain * fold).astype(BF).reshape(tok_rows, q_heads, width)
    lane_pair = lax.broadcasted_iota(jnp.int32, (1, width), 1) // HEAD_DIM
    q_rows = jnp.concatenate(
        [
            jnp.where(lane_pair == p, q_normed[:, h], jnp.zeros((), BF))
            for h in range(q_heads)
            for p in range(2)
        ],
        axis=0,
    )
    sums = attend(q_rows, kv, 2048, q_rows.shape[0] // 2, 256)
    sums = sums.reshape(q_heads, 2, tok_rows, 2 * width)
    ratio = sums[..., :width] / sums[..., width:]
    difference = ratio[:, 0] - lambdas.reshape(q_heads, 1, 1) * ratio[:, 1]
    att = (rms_scale(difference, head_gain) * (1.0 - LAMBDA_INIT)).astype(BF)

    glu_rows = (project(wgv) * jax.nn.sigmoid(project(wgg))).astype(BF)
    reach = CONV_W // 2
    count = lax.axis_size("sp")
    up = [(i, i + 1) for i in range(count - 1)]
    padded = jnp.concatenate(
        [
            lax.ppermute(glu_rows[tok_rows - reach :], "sp", up),
            glu_rows,
            lax.ppermute(glu_rows[:reach], "sp", [(b, a) for a, b in up]),
        ],
        axis=0,
    )
    conv_sum = jnp.zeros((tok_rows, glu_rows.shape[1]), F32)
    for offset in range(CONV_W):
        conv_sum = conv_sum + conv_weight[offset] * padded[offset : offset + tok_rows].astype(F32)
    partial_squares = jnp.sum(conv_sum * conv_sum, axis=1)
    eight = lax.axis_size("x") * lax.axis_size("c")
    squares = jnp.sum(
        lax.all_to_all(
            jnp.broadcast_to(partial_squares, (eight, tok_rows)), TP, 0, 0, tiled=True
        ),
        axis=0,
    )
    scaled = conv_sum * lax.rsqrt(squares / C_CH + EPS)[:, None] * channel_gain
    conv_out = jax.nn.silu(scaled).astype(BF)

    term = contract_last(conv_out, wco)
    for h in range(q_heads):
        term = term + contract_last(att[h], wao[:, h * width : (h + 1) * width])
    parts = term.astype(BF).reshape(eight, tok_rows // eight, term.shape[1])
    arrived = lax.all_to_all(parts, TP, 0, 0, tiled=True)
    return arrived.astype(F32).sum(axis=0).astype(BF)


def solution(mesh):
    finer = Mesh(mesh.devices.reshape(mesh.shape["sp"], 4, 2), SP_TP)
    both, rows = P("sp", TP), P()
    placed = (both, rows) + (both,) * 5 + (rows, rows, P(TP), rows, P(None, TP), P(TP), both, both)
    return jax.shard_map(
        local, mesh=finer, in_specs=placed, out_specs=P(SP_TP, None), check_vma=False
    )
```

```python
import functools
import math

import jax
import jax.numpy as jnp
from jax import lax
from jax.experimental import pallas as pl
from jax.experimental.pallas import tpu as pltpu
from jax.sharding import Mesh
from jax.sharding import PartitionSpec as P

HEAD_DIM = 64
WIDTH = 2 * HEAD_DIM
C_CH = 1536
CONV_W = 31
REACH = CONV_W // 2
EPS = 1e-06
LAMBDA_INIT = 0.2
BF = jnp.bfloat16
F32 = jnp.float32
TP = ("x", "c")
PLANE = ("y", "x", "c")
TOK_RING = ("z", "x", "c")


def rms_scale(values, gain):
    return values * lax.rsqrt(jnp.mean(values * values, axis=-1, keepdims=True) + EPS) * gain


def contract_last(left, right):
    return lax.dot_general(left, right, (((1,), (1,)), ((), ())), preferred_element_type=F32)


def copies_to(array, axis):
    copies = jnp.broadcast_to(array, (lax.axis_size(axis), *array.shape))
    return lax.all_to_all(copies, axis, 0, 0, tiled=True)


def diagonal(size):
    rows = lax.broadcasted_iota(jnp.int32, (size, size), 0)
    return rows == lax.broadcasted_iota(jnp.int32, (size, size), 1)


def attend_kernel(qs_ref, k0_ref, v0_ref, k1_ref, v1_ref, o_ref, acc_ref, q_ref, *, rows, keys):
    step = pl.program_id(0)

    @pl.when(step == 0)
    def _():
        acc_ref[...] = jnp.zeros_like(acc_ref)
        groups, tok, cols = qs_ref.shape
        pair = lax.broadcasted_iota(jnp.int32, (tok, WIDTH), 1) // HEAD_DIM
        at = 0
        for g in range(groups):
            for h in range(cols // WIDTH):
                q = qs_ref[g, :, h * WIDTH : (h + 1) * WIDTH].astype(F32)
                for p in range(2):
                    q_ref[at : at + tok, :] = jnp.where(pair == p, q, 0.0).astype(BF)
                    at += tok

    ones = jnp.ones((keys, WIDTH), BF)
    for k_ref, v_ref in ((k0_ref, v0_ref), (k1_ref, v1_ref)):
        for j in range(k_ref.shape[0] // keys):
            k = k_ref[j * keys : (j + 1) * keys, :]
            v = jnp.concatenate([v_ref[j * keys : (j + 1) * keys, :], ones], axis=1)
            for r in range(q_ref.shape[0] // rows):
                part = pl.ds(r * rows, rows)
                s = contract_last(q_ref[part, :], k)
                e = jnp.exp2(s).astype(BF)
                acc_ref[part, :] += jnp.dot(e, v, preferred_element_type=F32)

    @pl.when(step == pl.num_programs(0) - 1)
    def _():
        groups, padded, _ = o_ref.shape
        count = acc_ref.shape[0] // groups
        eye = diagonal(WIDTH)
        for g in range(groups):
            o_ref[g, :count, :] = acc_ref[g * count : (g + 1) * count, :WIDTH].astype(BF)
            lines = []
            for j in range(count // WIDTH):
                start = g * count + j * WIDTH
                block = acc_ref[start : start + WIDTH, WIDTH:]
                lines.append(jnp.sum(jnp.where(eye, block, 0.0), axis=0, keepdims=True))
            lines.append(jnp.zeros((8 - len(lines), WIDTH), F32))
            sums = jnp.concatenate(lines, axis=0)
            high = sums.astype(BF).astype(F32)
            both = jnp.concatenate([high, sums - high], axis=0)
            o_ref[g, count:padded, :] = both.astype(BF)


def attend(q_all, kv_own, kv_other, block, rows, keys):
    groups, tok, cols = q_all.shape
    each, total = 2 * tok * (cols // WIDTH), kv_own.shape[0]
    count = groups * each
    half = [pl.BlockSpec((block, WIDTH), lambda i, h=h: (i, h)) for h in (0, 1)]
    return pl.pallas_call(
        functools.partial(attend_kernel, rows=rows, keys=keys),
        grid=(total // block,),
        in_specs=[pl.BlockSpec(q_all.shape, lambda i: (0, 0, 0))] + half + half,
        out_specs=pl.BlockSpec((groups, each + 16, WIDTH), lambda i: (0, 0, 0)),
        out_shape=jax.ShapeDtypeStruct((groups, each + 16, WIDTH), BF),
        scratch_shapes=[pltpu.VMEM((count, 2 * WIDTH), F32), pltpu.VMEM((count, WIDTH), BF)],
        cost_estimate=pl.CostEstimate(
            flops=12 * count * total * WIDTH,
            transcendentals=2 * count * total,
            bytes_accessed=total * 8 * WIDTH + count * 4 * WIDTH,
        ),
        name="attend",
    )(q_all, kv_own, kv_own, kv_other, kv_other)


def combine_kernel(parts_ref, lam_ref, gain_ref, out_ref, ratio_ref):
    count = parts_ref.shape[1] - 16
    total = parts_ref[0].astype(F32)
    for g in range(1, parts_ref.shape[0]):
        total = total + parts_ref[g].astype(F32)
    sums = total[count : count + 8] + total[count + 8 : count + 16]
    eye = diagonal(WIDTH)
    for j in range(count // WIDTH):
        line = jnp.broadcast_to(sums[j : j + 1], (WIDTH, WIDTH))
        column = jnp.sum(jnp.where(eye, line, 0.0), axis=1, keepdims=True)
        ratio_ref[j * WIDTH : (j + 1) * WIDTH, :] = total[j * WIDTH : (j + 1) * WIDTH] / column
    tok = out_ref.shape[0]
    for h in range(out_ref.shape[1] // WIDTH):
        start = 2 * h * tok
        first = ratio_ref[start : start + tok, :]
        second = ratio_ref[start + tok : start + 2 * tok, :]
        o = first - lam_ref[h : h + 1, :] * second
        o = rms_scale(o, gain_ref[...]) * (1.0 - LAMBDA_INIT)
        out_ref[:, h * WIDTH : (h + 1) * WIDTH] = o.astype(BF)


def combine(parts, lam, gain, tok, heads):
    count = parts.shape[1] - 16
    lam_rows = jnp.broadcast_to(jnp.pad(lam, (0, 8 - heads))[:, None], (8, WIDTH))
    return pl.pallas_call(
        combine_kernel,
        out_shape=jax.ShapeDtypeStruct((tok, heads * WIDTH), BF),
        scratch_shapes=[pltpu.VMEM((count, WIDTH), F32)],
        name="combine",
    )(parts, lam_rows, gain.reshape(1, WIDTH))


def local(
    tokens,
    norm_gain,
    query_weight,
    key_weight,
    value_weight,
    glu_value_weight,
    glu_gate_weight,
    query_gain,
    key_gain,
    lambdas,
    head_gain,
    conv_weight,
    channel_gain,
    attn_out_weight,
    conv_out_weight,
):
    n = lax.axis_size("y")
    heads = query_weight.shape[1] // WIDTH
    tok = tokens.shape[0]
    seg = tok // n
    channels = conv_weight.shape[1]

    swap = [(y * n + t, t * n + y) for y in range(n) for t in range(n)]
    weights = (query_weight, key_weight, value_weight, glu_value_weight, glu_gate_weight)
    weights = weights + (attn_out_weight, conv_out_weight)
    first = sum(w.shape[1] for w in weights[:3])
    shard = lax.ppermute(jnp.concatenate(weights, axis=1), PLANE, swap)
    small = jnp.concatenate(
        [
            conv_weight,
            channel_gain[None],
            jnp.pad(lambdas, (0, channels - heads))[None],
            jnp.zeros((7, channels), F32),
        ],
        axis=0,
    )
    small = lax.ppermute(small, PLANE, swap)
    conv_weight, channel_gain = small[:CONV_W], small[CONV_W]
    lambdas = small[CONV_W + 1, :heads]

    blocks = tokens.reshape(n, seg, tokens.shape[1])
    blocks = jnp.broadcast_to(blocks, (n, *blocks.shape)).reshape(n * n, seg, -1)
    mine = lax.all_to_all(blocks, PLANE, 0, 0, tiled=True)
    mine = mine.reshape(n, n, seg, -1)
    gathered = mine.transpose(0, 2, 1, 3).reshape(n, seg, -1).astype(F32)
    normed = rms_scale(gathered, norm_gain).astype(BF).reshape(tok, -1)

    by_z = lax.all_gather(shard, "z", axis=0)
    core = lax.axis_index("c")

    def whole(columns):
        rows = columns.reshape(-1, columns.shape[-1])
        own = copies_to(rows, "x")
        other = lax.ppermute(own, "c", [(0, 1), (1, 0)])
        both = jnp.stack([jnp.where(core == 0, own, other), jnp.where(core == 0, other, own)])
        both = both.reshape(2, 4, n, shard.shape[0], -1)
        return both.transpose(2, 1, 0, 3, 4).reshape(-1, columns.shape[-1])

    w_first = whole(by_z[..., :first])

    def project(w):
        return jnp.dot(normed, w, preferred_element_type=F32)

    q_cols, k_cols = query_weight.shape[1], key_weight.shape[1]
    keys = project(w_first[:, q_cols : q_cols + k_cols]).reshape(tok, -1, HEAD_DIM)
    key_rows = rms_scale(keys, key_gain).astype(BF).reshape(tok, k_cols)
    value_rows = project(w_first[:, q_cols + k_cols :]).astype(BF)
    kv = copies_to(jnp.concatenate([key_rows, value_rows], axis=1), "z")
    kv = kv.reshape(-1, kv.shape[-1])
    kv_other = lax.ppermute(kv, "c", [(0, 1), (1, 0)])
    w_rest = whole(by_z[..., first:])

    fold = math.log2(math.e) * HEAD_DIM ** (-0.5)
    queries = project(w_first[:, :q_cols]).reshape(tok, -1, HEAD_DIM)
    q_normed = rms_scale(queries, query_gain * fold).astype(BF).reshape(tok, q_cols)
    q_all = lax.all_gather(q_normed, "x", axis=0)
    parts = attend(q_all, kv, kv_other, 256, 896, 256)
    arrived = lax.all_to_all(parts, "x", 0, 0, tiled=True)
    att = combine(arrived, lambdas, head_gain, tok, heads)

    g_cols = glu_value_weight.shape[1]
    glu_value = project(w_rest[:, :g_cols])
    glu_gate = project(w_rest[:, g_cols : 2 * g_cols])
    glu = (glu_value * jax.nn.sigmoid(glu_gate)).astype(BF).reshape(n, seg, g_cols)
    size_z = lax.axis_size("z")
    t = lax.axis_index(TP)
    heads_rows, tails = glu[:, :REACH], glu[:, seg - REACH :]
    ring = [(i, (i + 1) % n) for i in range(n)]
    left = lax.ppermute(tails, TP, ring)
    right = lax.ppermute(heads_rows, TP, [(b, a) for a, b in ring])
    across = [(z * n + n - 1, (z + 1) * n) for z in range(size_z - 1)]
    before = lax.ppermute(tails[n - 1 :], TOK_RING, across)
    after = lax.ppermute(heads_rows[:1], TOK_RING, [(b, a) for a, b in across])
    left = jnp.where(t == 0, jnp.concatenate([before, left[:-1]], axis=0), left)
    right = jnp.where(t == n - 1, jnp.concatenate([right[1:], after], axis=0), right)
    padded = jnp.concatenate([left, glu, right], axis=1)
    conv_sum = jnp.zeros((n, seg, g_cols), F32)
    for offset in range(CONV_W):
        conv_sum = conv_sum + conv_weight[offset] * padded[:, offset : offset + seg].astype(F32)
    squares = jnp.sum(conv_sum * conv_sum, axis=2)
    for bit in (1, 2, 4):
        moved = lax.ppermute(squares, "y", [(i, i ^ bit) for i in range(n)])
        squares = squares + moved
    scaled = conv_sum * lax.rsqrt(squares / C_CH + EPS)[..., None] * channel_gain
    conv_out = jax.nn.silu(scaled).astype(BF).reshape(tok, g_cols)

    w_out = w_rest[:, 2 * g_cols :]
    term = contract_last(att, w_out[:, : att.shape[1]])
    term = term + contract_last(conv_out, w_out[:, att.shape[1] :])
    term = term.astype(BF).reshape(n, seg, -1)
    reduced = lax.all_to_all(term, "y", 0, 0, tiled=True)
    return reduced.astype(F32).sum(axis=0).astype(BF)


def solution(mesh):
    finer = Mesh(mesh.devices.reshape(8, 8, 4, 2), ("z", "y", "x", "c"))
    sp = ("z", "y")
    both, rows = P(sp, TP), P()
    placed = (both, rows) + (both,) * 5 + (rows, rows, P(TP), rows, P(None, TP), P(TP), both, both)
    return jax.shard_map(
        local, mesh=finer, in_specs=placed, out_specs=P(sp + TP, None), check_vma=False
    )
```

```python
import functools
import math

import jax
import jax.numpy as jnp
from jax import lax
from jax.experimental import pallas as pl
from jax.experimental.pallas import tpu as pltpu
from jax.sharding import Mesh
from jax.sharding import PartitionSpec as P

HEAD_DIM = 64
WIDTH = 2 * HEAD_DIM
C_CH = 1536
CONV_W = 31
REACH = CONV_W // 2
EPS = 1e-06
LAMBDA_INIT = 0.2
BF = jnp.bfloat16
F32 = jnp.float32
TP = ("x", "c")
PLANE = ("y", "x", "c")
TOK_RING = ("z", "x", "c")


def rms_scale(values, gain):
    return values * lax.rsqrt(jnp.mean(values * values, axis=-1, keepdims=True) + EPS) * gain


def contract_last(left, right):
    return lax.dot_general(left, right, (((1,), (1,)), ((), ())), preferred_element_type=F32)


def copies_to(array, axis):
    copies = jnp.broadcast_to(array, (lax.axis_size(axis), *array.shape))
    return lax.all_to_all(copies, axis, 0, 0, tiled=True)


def diagonal(size):
    rows = lax.broadcasted_iota(jnp.int32, (size, size), 0)
    return rows == lax.broadcasted_iota(jnp.int32, (size, size), 1)


def attend_kernel(
    qs_ref, k0_ref, v0_ref, k1_ref, v1_ref, o_ref, acc_ref, q_ref, *, tok, rows, keys
):
    step = pl.program_id(0)

    @pl.when(step == 0)
    def _():
        acc_ref[...] = jnp.zeros_like(acc_ref)
        groups = qs_ref.shape[0]
        pair = lax.broadcasted_iota(jnp.int32, (tok, WIDTH), 1) // HEAD_DIM
        at = 0
        for g in range(groups):
            for h in range(qs_ref.shape[2] // WIDTH):
                q = qs_ref[g, :tok, h * WIDTH : (h + 1) * WIDTH].astype(F32)
                for p in range(2):
                    q_ref[at : at + tok, :] = jnp.where(pair == p, q, 0.0).astype(BF)
                    at += tok

    ones = jnp.ones((keys, WIDTH), BF)
    for k_ref, v_ref in ((k0_ref, v0_ref), (k1_ref, v1_ref)):
        for j in range(k_ref.shape[0] // keys):
            k = k_ref[j * keys : (j + 1) * keys, :]
            v = jnp.concatenate([v_ref[j * keys : (j + 1) * keys, :], ones], axis=1)
            for r in range(q_ref.shape[0] // rows):
                part = pl.ds(r * rows, rows)
                s = contract_last(q_ref[part, :], k)
                e = jnp.exp2(s).astype(BF)
                acc_ref[part, :] += jnp.dot(e, v, preferred_element_type=F32)

    @pl.when(step == pl.num_programs(0) - 1)
    def _():
        groups, padded, _ = o_ref.shape
        count = acc_ref.shape[0] // groups
        eye = diagonal(WIDTH)
        for g in range(groups):
            o_ref[g, :count, :] = acc_ref[g * count : (g + 1) * count, :WIDTH].astype(BF)
            lines = []
            for j in range(count // WIDTH):
                start = g * count + j * WIDTH
                block = acc_ref[start : start + WIDTH, WIDTH:]
                lines.append(jnp.sum(jnp.where(eye, block, 0.0), axis=0, keepdims=True))
            lines.append(jnp.zeros((8 - len(lines), WIDTH), F32))
            sums = jnp.concatenate(lines, axis=0)
            high = sums.astype(BF).astype(F32)
            both = jnp.concatenate([high, sums - high], axis=0)
            o_ref[g, count:padded, :] = both.astype(BF)


def attend(packed, tok, cols, kv_own, kv_other, block, rows, keys):
    groups = packed.shape[0]
    each, total = 2 * tok * (cols // WIDTH), kv_own.shape[0]
    count = groups * each
    half = [pl.BlockSpec((block, WIDTH), lambda i, h=h: (i, h)) for h in (0, 1)]
    return pl.pallas_call(
        functools.partial(attend_kernel, tok=tok, rows=rows, keys=keys),
        grid=(total // block,),
        in_specs=[pl.BlockSpec((groups, packed.shape[1], cols), lambda i: (0, 0, 0))] + half + half,
        out_specs=pl.BlockSpec((groups, each + 16, WIDTH), lambda i: (0, 0, 0)),
        out_shape=jax.ShapeDtypeStruct((groups, each + 16, WIDTH), BF),
        scratch_shapes=[pltpu.VMEM((count, 2 * WIDTH), F32), pltpu.VMEM((count, WIDTH), BF)],
        cost_estimate=pl.CostEstimate(
            flops=12 * count * total * WIDTH,
            transcendentals=2 * count * total,
            bytes_accessed=total * 8 * WIDTH + count * 4 * WIDTH,
        ),
        name="attend",
    )(packed, kv_own, kv_own, kv_other, kv_other)


def combine_kernel(parts_ref, lam_ref, gain_ref, out_ref, ratio_ref):
    count = parts_ref.shape[1] - 16
    total = parts_ref[0].astype(F32)
    for g in range(1, parts_ref.shape[0]):
        total = total + parts_ref[g].astype(F32)
    sums = total[count : count + 8] + total[count + 8 : count + 16]
    eye = diagonal(WIDTH)
    for j in range(count // WIDTH):
        line = jnp.broadcast_to(sums[j : j + 1], (WIDTH, WIDTH))
        column = jnp.sum(jnp.where(eye, line, 0.0), axis=1, keepdims=True)
        ratio_ref[j * WIDTH : (j + 1) * WIDTH, :] = total[j * WIDTH : (j + 1) * WIDTH] / column
    tok = out_ref.shape[0]
    for h in range(out_ref.shape[1] // WIDTH):
        start = 2 * h * tok
        first = ratio_ref[start : start + tok, :]
        second = ratio_ref[start + tok : start + 2 * tok, :]
        o = first - lam_ref[h : h + 1, :] * second
        o = rms_scale(o, gain_ref[...]) * (1.0 - LAMBDA_INIT)
        out_ref[:, h * WIDTH : (h + 1) * WIDTH] = o.astype(BF)


def combine(parts, lam, gain, tok, heads):
    count = parts.shape[1] - 16
    lam_rows = jnp.broadcast_to(jnp.pad(lam, (0, 8 - heads))[:, None], (8, WIDTH))
    return pl.pallas_call(
        combine_kernel,
        out_shape=jax.ShapeDtypeStruct((tok, heads * WIDTH), BF),
        scratch_shapes=[pltpu.VMEM((count, WIDTH), F32)],
        name="combine",
    )(parts, lam_rows, gain.reshape(1, WIDTH))


def natural_rows(core, own_ref, other_ref, z, cols):
    blocks = []
    for x in range(own_ref.shape[0]):
        own = own_ref[x, 32 * z : 32 * z + 32, cols]
        other = other_ref[x, 32 * z : 32 * z + 32, cols]
        blocks.append(jnp.where(core == 0, own, other))
        blocks.append(jnp.where(core == 0, other, own))
    return jnp.concatenate(blocks, axis=0)


def project(core, x_ref, own_ref, other_ref, cols):
    acc = None
    for z in range(own_ref.shape[1] // 32):
        rhs = natural_rows(core, own_ref, other_ref, z, cols)
        part = jnp.dot(x_ref[:, 256 * z : 256 * z + 256], rhs, preferred_element_type=F32)
        acc = part if acc is None else acc + part
    return acc


def qkv_kernel(core_ref, x_ref, own_ref, other_ref, qg_ref, kg_ref, q_ref, kv_ref):
    acc = project(core_ref[0], x_ref, own_ref, other_ref, slice(0, own_ref.shape[2]))
    low = lax.broadcasted_iota(jnp.int32, (x_ref.shape[0], WIDTH), 1) < HEAD_DIM

    def normed(block, gain):
        squares = block * block
        first = jnp.sum(jnp.where(low, squares, 0.0), axis=1, keepdims=True)
        second = jnp.sum(jnp.where(low, 0.0, squares), axis=1, keepdims=True)
        first = lax.rsqrt(first / HEAD_DIM + EPS)
        second = lax.rsqrt(second / HEAD_DIM + EPS)
        return (block * jnp.where(low, first, second) * gain).astype(BF)

    q_cols = q_ref.shape[1]
    for at in range(0, q_cols, WIDTH):
        q_ref[:, at : at + WIDTH] = normed(acc[:, at : at + WIDTH], qg_ref[...])
    kv_ref[:, :WIDTH] = normed(acc[:, q_cols : q_cols + WIDTH], kg_ref[...])
    kv_ref[:, WIDTH:] = acc[:, q_cols + WIDTH :].astype(BF)


SMEM = pl.BlockSpec(memory_space=pltpu.SMEM)
VMEM = pl.BlockSpec(memory_space=pltpu.VMEM)


def qkv(core, x, own, other, query_gain, key_gain):
    tok, q_cols = x.shape[0], own.shape[2] - 2 * WIDTH
    return pl.pallas_call(
        qkv_kernel,
        in_specs=[SMEM] + [VMEM] * 5,
        out_specs=[VMEM, VMEM],
        out_shape=[
            jax.ShapeDtypeStruct((tok, q_cols), BF),
            jax.ShapeDtypeStruct((tok, 2 * WIDTH), BF),
        ],
        name="qkv",
    )(core, x, own, other, jnp.tile(query_gain, 2)[None], jnp.tile(key_gain, 2)[None])


def glu_kernel(core_ref, x_ref, own_ref, other_ref, out_ref, *, start):
    channels = out_ref.shape[2]
    cols = slice(start, start + 2 * channels)
    acc = project(core_ref[0], x_ref, own_ref, other_ref, cols)
    value, gate = acc[:, :channels], acc[:, channels:]
    glu = value * (1.0 / (1.0 + jnp.exp(-gate)))
    seg = out_ref.shape[1]
    for y in range(out_ref.shape[0]):
        out_ref[y] = glu[seg * y : seg * y + seg].astype(BF)


def glu_of(core, x, own, other, start, channels, n):
    return pl.pallas_call(
        functools.partial(glu_kernel, start=start),
        in_specs=[SMEM] + [VMEM] * 3,
        out_specs=VMEM,
        out_shape=jax.ShapeDtypeStruct((n, x.shape[0] // n, channels), BF),
        name="glu",
    )(core, x, own, other)


def out_kernel(core_ref, att_ref, conv_ref, own_ref, other_ref, out_ref, *, start):
    cols = slice(start, own_ref.shape[2])
    act = jnp.concatenate([att_ref[...], conv_ref[...]], axis=1)
    seg = out_ref.shape[1]
    for z in range(own_ref.shape[1] // 32):
        rhs = natural_rows(core_ref[0], own_ref, other_ref, z, cols)
        term = contract_last(act, rhs)
        for y in range(out_ref.shape[0]):
            block = term[seg * y : seg * y + seg]
            out_ref[y, :, 256 * z : 256 * z + 256] = block.astype(BF)


def out_of(core, att, conv, own, other, start, n):
    width = own.shape[0] * own.shape[1] * 2
    return pl.pallas_call(
        functools.partial(out_kernel, start=start),
        in_specs=[SMEM] + [VMEM] * 4,
        out_specs=VMEM,
        out_shape=jax.ShapeDtypeStruct((n, att.shape[0] // n, width), BF),
        name="out",
    )(core, att, conv, own, other)


def local(
    tokens,
    norm_gain,
    query_weight,
    key_weight,
    value_weight,
    glu_value_weight,
    glu_gate_weight,
    query_gain,
    key_gain,
    lambdas,
    head_gain,
    conv_weight,
    channel_gain,
    attn_out_weight,
    conv_out_weight,
):
    n = lax.axis_size("y")
    heads = query_weight.shape[1] // WIDTH
    tok = tokens.shape[0]
    seg = tok // n
    channels = conv_weight.shape[1]

    swap = [(y * n + t, t * n + y) for y in range(n) for t in range(n)]
    weights = (query_weight, key_weight, value_weight, glu_value_weight, glu_gate_weight)
    weights = weights + (attn_out_weight, conv_out_weight)
    first = sum(w.shape[1] for w in weights[:3])
    shard = lax.ppermute(jnp.concatenate(weights, axis=1), PLANE, swap)
    small = jnp.concatenate(
        [
            conv_weight,
            channel_gain[None],
            jnp.pad(lambdas, (0, channels - heads))[None],
            jnp.zeros((7, channels), F32),
        ],
        axis=0,
    )
    small = lax.ppermute(small, PLANE, swap)
    conv_weight, channel_gain = small[:CONV_W], small[CONV_W]
    lambdas = small[CONV_W + 1, :heads]

    blocks = tokens.reshape(n, seg, tokens.shape[1])
    blocks = jnp.broadcast_to(blocks, (n, *blocks.shape)).reshape(n * n, seg, -1)
    mine = lax.all_to_all(blocks, PLANE, 0, 0, tiled=True)
    mine = mine.reshape(n, n, seg, -1)
    gathered = mine.transpose(0, 2, 1, 3).reshape(n, seg, -1).astype(F32)
    normed = rms_scale(gathered, norm_gain).astype(BF).reshape(tok, -1)

    by_z = lax.all_gather(shard, "z", axis=0)
    core = lax.axis_index("c").astype(jnp.int32)[None]
    mates = [(0, 1), (1, 0)]
    by_z = by_z.reshape(-1, by_z.shape[2])
    wa = copies_to(by_z[:, :first], "x")
    wa_other = lax.ppermute(wa, "c", mates)
    fold = math.log2(math.e) * HEAD_DIM ** (-0.5)
    q, kv = qkv(core, normed, wa, wa_other, query_gain * fold, key_gain)

    q_cols = q.shape[1]
    rest = jnp.concatenate(
        [jnp.pad(q, ((0, by_z.shape[0] - tok), (0, 0))), by_z[:, first:]], axis=1
    )
    rest = copies_to(rest, "x")
    kv = lax.all_gather(kv, "z", axis=0, tiled=True)
    kv_other = lax.ppermute(kv, "c", mates)
    rest_other = lax.ppermute(rest, "c", mates)
    parts = attend(rest, tok, q_cols, kv, kv_other, 256, 896, 256)
    arrived = lax.all_to_all(parts, "x", 0, 0, tiled=True)
    att = combine(arrived, lambdas, head_gain, tok, heads)

    g_cols = glu_value_weight.shape[1]
    glu = glu_of(core, normed, rest, rest_other, q_cols, g_cols, n)
    size_z = lax.axis_size("z")
    t = lax.axis_index(TP)
    heads_rows, tails = glu[:, :REACH], glu[:, seg - REACH :]
    ring = [(i, (i + 1) % n) for i in range(n)]
    left = lax.ppermute(tails, TP, ring)
    right = lax.ppermute(heads_rows, TP, [(b, a) for a, b in ring])
    across = [(z * n + n - 1, (z + 1) * n) for z in range(size_z - 1)]
    across = [(z * n + n - 1, (z + 1) * n) for z in range(size_z - 1)]
    across = across + [(b, a) for a, b in across]
    edge = jnp.where(t == 0, heads_rows[:1], tails[n - 1 :])
    edge = lax.ppermute(edge, TOK_RING, across)
    left = jnp.where(t == 0, jnp.concatenate([edge, left[:-1]], axis=0), left)
    right = jnp.where(t == n - 1, jnp.concatenate([right[1:], edge], axis=0), right)
    padded = jnp.concatenate([left, glu, right], axis=1)
    conv_sum = jnp.zeros((n, seg, g_cols), F32)
    for offset in range(CONV_W):
        conv_sum = conv_sum + conv_weight[offset] * padded[:, offset : offset + seg].astype(F32)
    squares = jnp.sum(conv_sum * conv_sum, axis=2)
    squares = jnp.sum(copies_to(squares, "y"), axis=0)
    scaled = conv_sum * lax.rsqrt(squares / C_CH + EPS)[..., None] * channel_gain
    conv_out = jax.nn.silu(scaled).astype(BF).reshape(tok, g_cols)

    term = out_of(core, att, conv_out, rest, rest_other, q_cols + 2 * g_cols, n)
    reduced = lax.all_to_all(term, "y", 0, 0, tiled=True)
    return reduced.astype(F32).sum(axis=0).astype(BF)


def solution(mesh):
    finer = Mesh(mesh.devices.reshape(8, 8, 4, 2), ("z", "y", "x", "c"))
    sp = ("z", "y")
    both, rows = P(sp, TP), P()
    placed = (both, rows) + (both,) * 5 + (rows, rows, P(TP), rows, P(None, TP), P(TP), both, both)
    return jax.shard_map(
        local, mesh=finer, in_specs=placed, out_specs=P(sp + TP, None), check_vma=False
    )
```

```python
import functools
import math

import jax
import jax.numpy as jnp
from jax import lax
from jax.experimental import pallas as pl
from jax.experimental.pallas import tpu as pltpu
from jax.sharding import Mesh
from jax.sharding import PartitionSpec as P

HEAD_DIM = 64
WIDTH = 2 * HEAD_DIM
C_CH = 1536
CONV_W = 31
REACH = CONV_W // 2
EPS = 1e-06
LAMBDA_INIT = 0.2
BF = jnp.bfloat16
F32 = jnp.float32
TP = ("x", "c")
PLANE = ("y", "x", "c")
TOK_RING = ("z", "x", "c")


def rms_scale(values, gain):
    return values * lax.rsqrt(jnp.mean(values * values, axis=-1, keepdims=True) + EPS) * gain


def contract_last(left, right):
    return lax.dot_general(left, right, (((1,), (1,)), ((), ())), preferred_element_type=F32)


def copies_to(array, axis):
    copies = jnp.broadcast_to(array, (lax.axis_size(axis), *array.shape))
    return lax.all_to_all(copies, axis, 0, 0, tiled=True)


def diagonal(size):
    rows = lax.broadcasted_iota(jnp.int32, (size, size), 0)
    return rows == lax.broadcasted_iota(jnp.int32, (size, size), 1)


def attend_kernel(
    qs_ref, k0_ref, v0_ref, k1_ref, v1_ref, o_ref, acc_ref, q_ref, *, tok, rows, keys
):
    step = pl.program_id(0)

    @pl.when(step == 0)
    def _():
        acc_ref[...] = jnp.zeros_like(acc_ref)
        groups = qs_ref.shape[0]
        pair = lax.broadcasted_iota(jnp.int32, (tok, WIDTH), 1) // HEAD_DIM
        at = 0
        for g in range(groups):
            for h in range(qs_ref.shape[2] // WIDTH):
                q = qs_ref[g, :tok, h * WIDTH : (h + 1) * WIDTH].astype(F32)
                for p in range(2):
                    q_ref[at : at + tok, :] = jnp.where(pair == p, q, 0.0).astype(BF)
                    at += tok

    ones = jnp.ones((keys, WIDTH), BF)
    for k_ref, v_ref in ((k0_ref, v0_ref), (k1_ref, v1_ref)):
        for j in range(k_ref.shape[0] // keys):
            k = k_ref[j * keys : (j + 1) * keys, :]
            v = jnp.concatenate([v_ref[j * keys : (j + 1) * keys, :], ones], axis=1)
            for r in range(q_ref.shape[0] // rows):
                part = pl.ds(r * rows, rows)
                s = contract_last(q_ref[part, :], k)
                e = jnp.exp2(s).astype(BF)
                acc_ref[part, :] += jnp.dot(e, v, preferred_element_type=F32)

    @pl.when(step == pl.num_programs(0) - 1)
    def _():
        groups, padded, _ = o_ref.shape
        count = acc_ref.shape[0] // groups
        eye = diagonal(WIDTH)
        for g in range(groups):
            o_ref[g, :count, :] = acc_ref[g * count : (g + 1) * count, :WIDTH].astype(BF)
            lines = []
            for j in range(count // WIDTH):
                start = g * count + j * WIDTH
                block = acc_ref[start : start + WIDTH, WIDTH:]
                lines.append(jnp.sum(jnp.where(eye, block, 0.0), axis=0, keepdims=True))
            lines.append(jnp.zeros((8 - len(lines), WIDTH), F32))
            sums = jnp.concatenate(lines, axis=0)
            high = sums.astype(BF).astype(F32)
            both = jnp.concatenate([high, sums - high], axis=0)
            o_ref[g, count:padded, :] = both.astype(BF)


def attend(packed, tok, cols, kv_own, kv_other, block, rows, keys):
    groups = packed.shape[0]
    each, total = 2 * tok * (cols // WIDTH), kv_own.shape[0]
    count = groups * each
    half = [pl.BlockSpec((block, WIDTH), lambda i, h=h: (i, h)) for h in (0, 1)]
    return pl.pallas_call(
        functools.partial(attend_kernel, tok=tok, rows=rows, keys=keys),
        grid=(total // block,),
        in_specs=[pl.BlockSpec((groups, packed.shape[1], cols), lambda i: (0, 0, 0))] + half + half,
        out_specs=pl.BlockSpec((groups, each + 16, WIDTH), lambda i: (0, 0, 0)),
        out_shape=jax.ShapeDtypeStruct((groups, each + 16, WIDTH), BF),
        scratch_shapes=[pltpu.VMEM((count, 2 * WIDTH), F32), pltpu.VMEM((count, WIDTH), BF)],
        cost_estimate=pl.CostEstimate(
            flops=12 * count * total * WIDTH,
            transcendentals=2 * count * total,
            bytes_accessed=total * 8 * WIDTH + count * 4 * WIDTH,
        ),
        name="attend",
    )(packed, kv_own, kv_own, kv_other, kv_other)


def combine_kernel(parts_ref, lam_ref, gain_ref, out_ref, ratio_ref):
    count = parts_ref.shape[1] - 16
    total = parts_ref[0].astype(F32)
    for g in range(1, parts_ref.shape[0]):
        total = total + parts_ref[g].astype(F32)
    sums = total[count : count + 8] + total[count + 8 : count + 16]
    eye = diagonal(WIDTH)
    for j in range(count // WIDTH):
        line = jnp.broadcast_to(sums[j : j + 1], (WIDTH, WIDTH))
        column = jnp.sum(jnp.where(eye, line, 0.0), axis=1, keepdims=True)
        ratio_ref[j * WIDTH : (j + 1) * WIDTH, :] = total[j * WIDTH : (j + 1) * WIDTH] / column
    tok = out_ref.shape[0]
    for h in range(out_ref.shape[1] // WIDTH):
        start = 2 * h * tok
        first = ratio_ref[start : start + tok, :]
        second = ratio_ref[start + tok : start + 2 * tok, :]
        o = first - lam_ref[h : h + 1, :] * second
        o = rms_scale(o, gain_ref[...]) * (1.0 - LAMBDA_INIT)
        out_ref[:, h * WIDTH : (h + 1) * WIDTH] = o.astype(BF)


def combine(parts, lam, gain, tok, heads):
    count = parts.shape[1] - 16
    lam_rows = jnp.broadcast_to(jnp.pad(lam, (0, 8 - heads))[:, None], (8, WIDTH))
    return pl.pallas_call(
        combine_kernel,
        out_shape=jax.ShapeDtypeStruct((tok, heads * WIDTH), BF),
        scratch_shapes=[pltpu.VMEM((count, WIDTH), F32)],
        name="combine",
    )(parts, lam_rows, gain.reshape(1, WIDTH))


def natural_rows(core, own_ref, other_ref, z, cols):
    blocks = []
    for x in range(own_ref.shape[0]):
        own = own_ref[x, 32 * z : 32 * z + 32, cols]
        other = other_ref[x, 32 * z : 32 * z + 32, cols]
        blocks.append(jnp.where(core == 0, own, other))
        blocks.append(jnp.where(core == 0, other, own))
    return jnp.concatenate(blocks, axis=0)


def project(core, x_ref, own_ref, other_ref, cols):
    acc = None
    for z in range(own_ref.shape[1] // 32):
        rhs = natural_rows(core, own_ref, other_ref, z, cols)
        part = jnp.dot(x_ref[:, 256 * z : 256 * z + 256], rhs, preferred_element_type=F32)
        acc = part if acc is None else acc + part
    return acc


def qkv_kernel(core_ref, x_ref, own_ref, other_ref, qg_ref, kg_ref, _, q_ref, kv_ref):
    acc = project(core_ref[0], x_ref, own_ref, other_ref, slice(0, own_ref.shape[2]))
    low = lax.broadcasted_iota(jnp.int32, (x_ref.shape[0], WIDTH), 1) < HEAD_DIM

    def normed(block, gain):
        squares = block * block
        first = jnp.sum(jnp.where(low, squares, 0.0), axis=1, keepdims=True)
        second = jnp.sum(jnp.where(low, 0.0, squares), axis=1, keepdims=True)
        first = lax.rsqrt(first / HEAD_DIM + EPS)
        second = lax.rsqrt(second / HEAD_DIM + EPS)
        return (block * jnp.where(low, first, second) * gain).astype(BF)

    tok, q_cols = x_ref.shape[0], q_ref.shape[2]
    for at in range(0, q_cols, WIDTH):
        q = normed(acc[:, at : at + WIDTH], qg_ref[...])
        for g in range(q_ref.shape[0]):
            q_ref[g, :tok, at : at + WIDTH] = q
    q_ref[:, tok:, :] = jnp.zeros((q_ref.shape[0], q_ref.shape[1] - tok, q_cols), BF)
    kv_ref[:, :WIDTH] = normed(acc[:, q_cols : q_cols + WIDTH], kg_ref[...])
    kv_ref[:, WIDTH:] = acc[:, q_cols + WIDTH :].astype(BF)


SMEM = pl.BlockSpec(memory_space=pltpu.SMEM)
VMEM = pl.BlockSpec(memory_space=pltpu.VMEM)


def qkv(core, x, own, other, query_gain, key_gain, packed):
    tok, q_cols = x.shape[0], own.shape[2] - 2 * WIDTH
    return pl.pallas_call(
        qkv_kernel,
        grid=(1,),
        in_specs=[SMEM] + [VMEM] * 5 + [pl.BlockSpec(memory_space=pl.ANY)],
        out_specs=[pl.BlockSpec((*packed.shape[:2], q_cols), lambda i: (0, 0, 0)), VMEM],
        out_shape=[
            jax.ShapeDtypeStruct(packed.shape, BF),
            jax.ShapeDtypeStruct((tok, 2 * WIDTH), BF),
        ],
        input_output_aliases={6: 0},
        name="qkv",
    )(core, x, own, other, jnp.tile(query_gain, 2)[None], jnp.tile(key_gain, 2)[None], packed)


def glu_kernel(core_ref, x_ref, own_ref, other_ref, out_ref, *, start):
    channels = out_ref.shape[2]
    cols = slice(start, start + 2 * channels)
    acc = project(core_ref[0], x_ref, own_ref, other_ref, cols)
    value, gate = acc[:, :channels], acc[:, channels:]
    glu = value * (1.0 / (1.0 + jnp.exp(-gate)))
    seg = out_ref.shape[1]
    for y in range(out_ref.shape[0]):
        out_ref[y] = glu[seg * y : seg * y + seg].astype(BF)


def glu_of(core, x, own, other, start, channels, n):
    return pl.pallas_call(
        functools.partial(glu_kernel, start=start),
        in_specs=[SMEM] + [VMEM] * 3,
        out_specs=VMEM,
        out_shape=jax.ShapeDtypeStruct((n, x.shape[0] // n, channels), BF),
        name="glu",
    )(core, x, own, other)


def conv_kernel(
    t_ref, glu_ref, left_ref, right_ref, edge_ref, w_ref, sum_ref, sq_ref, pad_ref
):
    n, seg, _ = glu_ref.shape
    t = t_ref[0]
    for y in range(n):
        inner = edge_ref[0] if y == 0 else left_ref[y - 1]
        pad_ref[y, :REACH] = jnp.where(t == 0, inner, left_ref[y]).astype(F32)
        pad_ref[y, REACH : REACH + seg] = glu_ref[y].astype(F32)
        inner = edge_ref[0] if y == n - 1 else right_ref[y + 1]
        pad_ref[y, REACH + seg : 2 * REACH + seg] = jnp.where(
            t == n - 1, inner, right_ref[y]
        ).astype(F32)
    for y in range(n):
        acc = jnp.zeros((seg, glu_ref.shape[2]), F32)
        for j in range(CONV_W):
            acc = acc + w_ref[j : j + 1, :] * pad_ref[y, j : j + seg]
        sum_ref[y] = acc
        sq_ref[y] = jnp.sum(acc * acc, axis=1, keepdims=True)


def conv_of(t, glu, left, right, edge, weight):
    n, seg, channels = glu.shape
    return pl.pallas_call(
        conv_kernel,
        in_specs=[SMEM] + [VMEM] * 5,
        out_specs=[VMEM, VMEM],
        out_shape=[
            jax.ShapeDtypeStruct((n, seg, channels), F32),
            jax.ShapeDtypeStruct((n, seg, 1), F32),
        ],
        scratch_shapes=[pltpu.VMEM((n, 64, channels), F32)],
        name="conv",
    )(t, glu, left, right, edge, weight)


def out_kernel(core_ref, att_ref, conv_ref, own_ref, other_ref, out_ref, *, start):
    cols = slice(start, start + att_ref.shape[1] + conv_ref.shape[1])
    act = jnp.concatenate([att_ref[...], conv_ref[...]], axis=1)
    seg = out_ref.shape[1]
    for z in range(own_ref.shape[1] // 32):
        rhs = natural_rows(core_ref[0], own_ref, other_ref, z, cols)
        term = contract_last(act, rhs)
        for y in range(out_ref.shape[0]):
            block = term[seg * y : seg * y + seg]
            out_ref[y, :, 256 * z : 256 * z + 256] = block.astype(BF)


def out_of(core, att, conv, own, other, start, n):
    width = own.shape[0] * own.shape[1] * 2
    return pl.pallas_call(
        functools.partial(out_kernel, start=start),
        in_specs=[SMEM] + [VMEM] * 4,
        out_specs=VMEM,
        out_shape=jax.ShapeDtypeStruct((n, att.shape[0] // n, width), BF),
        name="out",
    )(core, att, conv, own, other)


def local(
    tokens,
    norm_gain,
    query_weight,
    key_weight,
    value_weight,
    glu_value_weight,
    glu_gate_weight,
    query_gain,
    key_gain,
    lambdas,
    head_gain,
    conv_weight,
    channel_gain,
    attn_out_weight,
    conv_out_weight,
):
    n = lax.axis_size("y")
    heads = query_weight.shape[1] // WIDTH
    tok = tokens.shape[0]
    seg = tok // n
    channels = conv_weight.shape[1]

    swap = [(y * n + t, t * n + y) for y in range(n) for t in range(n)]
    weights = (query_weight, key_weight, value_weight, glu_value_weight, glu_gate_weight)
    weights = weights + (attn_out_weight, conv_out_weight)
    first = sum(w.shape[1] for w in weights[:3])
    small = jnp.concatenate([conv_weight, channel_gain[None]], axis=0)
    lam = jnp.pad(lambdas[None], ((0, small.shape[0] - 1), (0, WIDTH - heads)))
    small = jnp.concatenate([small, lam], axis=1)
    terms = []
    for _ in range(3):
        term = lax.reduce_precision(small, 8, 7)
        small = small - term
        terms.append(term.astype(BF))
    columns = sum(w.shape[1] for w in weights)
    shard = lax.ppermute(jnp.concatenate(weights + tuple(terms), axis=1), PLANE, swap)
    span = channels + WIDTH
    small = sum(
        shard[:, columns + i * span : columns + (i + 1) * span].astype(F32) for i in (2, 1, 0)
    )
    shard = shard[:, :columns]
    conv_weight, channel_gain = small[:CONV_W, :channels], small[CONV_W, :channels]
    lambdas = small[0, channels : channels + heads]

    blocks = tokens.reshape(n, seg, tokens.shape[1])
    blocks = jnp.broadcast_to(blocks, (n, *blocks.shape)).reshape(n * n, seg, -1)
    mine = lax.all_to_all(blocks, PLANE, 0, 0, tiled=True)
    mine = mine.reshape(n, n, seg, -1)
    gathered = mine.transpose(0, 2, 1, 3).reshape(n, seg, -1).astype(F32)
    normed = rms_scale(gathered, norm_gain).astype(BF).reshape(tok, -1)

    by_z = lax.all_gather(shard, "z", axis=0)
    core = lax.axis_index("c").astype(jnp.int32)[None]
    mates = [(0, 1), (1, 0)]
    by_z = by_z.reshape(-1, by_z.shape[2])
    wa = copies_to(by_z[:, :first], "x")
    wa_other = lax.ppermute(wa, "c", mates)
    fold = math.log2(math.e) * HEAD_DIM ** (-0.5)
    q_cols = query_weight.shape[1]
    late = columns - first
    rest = jnp.pad(by_z[:, first:], ((0, 0), (q_cols, -(q_cols + late) % WIDTH)))
    rest = jnp.broadcast_to(rest, (lax.axis_size("x"), *rest.shape))
    rest, kv = qkv(core, normed, wa, wa_other, query_gain * fold, key_gain, rest)
    rest = lax.all_to_all(rest, "x", 0, 0, tiled=True)
    kv = lax.all_gather(kv, "z", axis=0, tiled=True)
    kv_other = lax.ppermute(kv, "c", mates)
    rest_other = lax.ppermute(rest, "c", mates)
    parts = attend(rest, tok, q_cols, kv, kv_other, 1792, 896, 256)
    arrived = lax.all_to_all(parts, "x", 0, 0, tiled=True)
    att = combine(arrived, lambdas, head_gain, tok, heads)

    g_cols = glu_value_weight.shape[1]
    glu = glu_of(core, normed, rest, rest_other, q_cols, g_cols, n)
    size_z = lax.axis_size("z")
    t = lax.axis_index(TP)
    heads_rows, tails = glu[:, :REACH], glu[:, seg - REACH :]
    ring = [(i, (i + 1) % n) for i in range(n)]
    left = lax.ppermute(tails, TP, ring)
    right = lax.ppermute(heads_rows, TP, [(b, a) for a, b in ring])
    across = [(z * n + n - 1, (z + 1) * n) for z in range(size_z - 1)]
    across = [(z * n + n - 1, (z + 1) * n) for z in range(size_z - 1)]
    across = across + [(b, a) for a, b in across]
    edge = jnp.where(t == 0, heads_rows[:1], tails[n - 1 :])
    edge = lax.ppermute(edge, TOK_RING, across)
    conv_sum, squares = conv_of(t.astype(jnp.int32)[None], glu, left, right, edge, conv_weight)
    squares = squares.reshape(n, seg)
    squares = jnp.sum(copies_to(squares, "y"), axis=0)
    scaled = conv_sum * lax.rsqrt(squares / C_CH + EPS)[..., None] * channel_gain
    conv_out = jax.nn.silu(scaled).astype(BF).reshape(tok, g_cols)

    term = out_of(core, att, conv_out, rest, rest_other, q_cols + 2 * g_cols, n)
    reduced = lax.all_to_all(term, "y", 0, 0, tiled=True)
    return reduced.astype(F32).sum(axis=0).astype(BF)


def solution(mesh):
    finer = Mesh(mesh.devices.reshape(8, 8, 4, 2), ("z", "y", "x", "c"))
    sp = ("z", "y")
    both, rows = P(sp, TP), P()
    placed = (both, rows) + (both,) * 5 + (rows, rows, P(TP), rows, P(None, TP), P(TP), both, both)
    return jax.shard_map(
        local, mesh=finer, in_specs=placed, out_specs=P(sp + TP, None), check_vma=False
    )
```

```python
import functools
import math

import jax
import jax.numpy as jnp
from jax import lax
from jax.experimental import pallas as pl
from jax.experimental.pallas import tpu as pltpu
from jax.sharding import Mesh
from jax.sharding import PartitionSpec as P

HEAD_DIM = 64
WIDTH = 2 * HEAD_DIM
C_CH = 1536
CONV_W = 31
REACH = CONV_W // 2
EPS = 1e-06
LAMBDA_INIT = 0.2
BF = jnp.bfloat16
F32 = jnp.float32
TP = ("x", "c")
PLANE = ("y", "x", "c")
TOK_RING = ("z", "x", "c")


def rms_scale(values, gain):
    return values * lax.rsqrt(jnp.mean(values * values, axis=-1, keepdims=True) + EPS) * gain


def contract_last(left, right):
    return lax.dot_general(left, right, (((1,), (1,)), ((), ())), preferred_element_type=F32)


def copies_to(array, axis):
    copies = jnp.broadcast_to(array, (lax.axis_size(axis), *array.shape))
    return lax.all_to_all(copies, axis, 0, 0, tiled=True)


def diagonal(size):
    rows = lax.broadcasted_iota(jnp.int32, (size, size), 0)
    return rows == lax.broadcasted_iota(jnp.int32, (size, size), 1)


def attend_kernel(
    qs_ref, k0_ref, v0_ref, k1_ref, v1_ref, o_ref, acc_ref, q_ref, *, tok, rows, keys
):
    step = pl.program_id(0)

    @pl.when(step == 0)
    def _():
        acc_ref[...] = jnp.zeros_like(acc_ref)
        groups = qs_ref.shape[0]
        pair = lax.broadcasted_iota(jnp.int32, (tok, WIDTH), 1) // HEAD_DIM
        at = 0
        for g in range(groups):
            for h in range(qs_ref.shape[2] // WIDTH):
                q = qs_ref[g, :tok, h * WIDTH : (h + 1) * WIDTH].astype(F32)
                for p in range(2):
                    q_ref[at : at + tok, :] = jnp.where(pair == p, q, 0.0).astype(BF)
                    at += tok

    ones = jnp.ones((keys, WIDTH), BF)
    for k_ref, v_ref in ((k0_ref, v0_ref), (k1_ref, v1_ref)):
        for j in range(k_ref.shape[0] // keys):
            k = k_ref[j * keys : (j + 1) * keys, :]
            v = jnp.concatenate([v_ref[j * keys : (j + 1) * keys, :], ones], axis=1)
            for r in range(q_ref.shape[0] // rows):
                part = pl.ds(r * rows, rows)
                s = contract_last(q_ref[part, :], k)
                e = jnp.exp2(s).astype(BF)
                acc_ref[part, :] += jnp.dot(e, v, preferred_element_type=F32)

    @pl.when(step == pl.num_programs(0) - 1)
    def _():
        groups, padded, _ = o_ref.shape
        count = acc_ref.shape[0] // groups
        eye = diagonal(WIDTH)
        for g in range(groups):
            o_ref[g, :count, :] = acc_ref[g * count : (g + 1) * count, :WIDTH].astype(BF)
            lines = []
            for j in range(count // WIDTH):
                start = g * count + j * WIDTH
                block = acc_ref[start : start + WIDTH, WIDTH:]
                lines.append(jnp.sum(jnp.where(eye, block, 0.0), axis=0, keepdims=True))
            lines.append(jnp.zeros((8 - len(lines), WIDTH), F32))
            sums = jnp.concatenate(lines, axis=0)
            high = sums.astype(BF).astype(F32)
            both = jnp.concatenate([high, sums - high], axis=0)
            o_ref[g, count:padded, :] = both.astype(BF)


def attend(packed, tok, cols, kv_own, kv_other, block, rows, keys):
    groups = packed.shape[0]
    each, total = 2 * tok * (cols // WIDTH), kv_own.shape[0]
    count = groups * each
    half = [pl.BlockSpec((block, WIDTH), lambda i, h=h: (i, h)) for h in (0, 1)]
    return pl.pallas_call(
        functools.partial(attend_kernel, tok=tok, rows=rows, keys=keys),
        grid=(total // block,),
        in_specs=[pl.BlockSpec((groups, packed.shape[1], cols), lambda i: (0, 0, 0))] + half + half,
        out_specs=pl.BlockSpec((groups, each + 16, WIDTH), lambda i: (0, 0, 0)),
        out_shape=jax.ShapeDtypeStruct((groups, each + 16, WIDTH), BF),
        scratch_shapes=[pltpu.VMEM((count, 2 * WIDTH), F32), pltpu.VMEM((count, WIDTH), BF)],
        cost_estimate=pl.CostEstimate(
            flops=12 * count * total * WIDTH,
            transcendentals=2 * count * total,
            bytes_accessed=total * 8 * WIDTH + count * 4 * WIDTH,
        ),
        name="attend",
    )(packed, kv_own, kv_own, kv_other, kv_other)


def combine_kernel(parts_ref, lam_ref, gain_ref, out_ref, ratio_ref):
    count = parts_ref.shape[1] - 16
    total = parts_ref[0].astype(F32)
    for g in range(1, parts_ref.shape[0]):
        total = total + parts_ref[g].astype(F32)
    sums = total[count : count + 8] + total[count + 8 : count + 16]
    eye = diagonal(WIDTH)
    for j in range(count // WIDTH):
        line = jnp.broadcast_to(sums[j : j + 1], (WIDTH, WIDTH))
        column = jnp.sum(jnp.where(eye, line, 0.0), axis=1, keepdims=True)
        ratio_ref[j * WIDTH : (j + 1) * WIDTH, :] = total[j * WIDTH : (j + 1) * WIDTH] / column
    tok = out_ref.shape[0]
    for h in range(out_ref.shape[1] // WIDTH):
        start = 2 * h * tok
        first = ratio_ref[start : start + tok, :]
        second = ratio_ref[start + tok : start + 2 * tok, :]
        o = first - lam_ref[h : h + 1, :] * second
        o = rms_scale(o, gain_ref[...]) * (1.0 - LAMBDA_INIT)
        out_ref[:, h * WIDTH : (h + 1) * WIDTH] = o.astype(BF)


def combine(parts, lam, gain, tok, heads):
    count = parts.shape[1] - 16
    lam_rows = jnp.broadcast_to(jnp.pad(lam, (0, 8 - heads))[:, None], (8, WIDTH))
    return pl.pallas_call(
        combine_kernel,
        out_shape=jax.ShapeDtypeStruct((tok, heads * WIDTH), BF),
        scratch_shapes=[pltpu.VMEM((count, WIDTH), F32)],
        name="combine",
    )(parts, lam_rows, gain.reshape(1, WIDTH))


def natural_rows(core, own_ref, other_ref, z, cols):
    blocks = []
    for x in range(own_ref.shape[0]):
        own = own_ref[x, 32 * z : 32 * z + 32, cols]
        other = other_ref[x, 32 * z : 32 * z + 32, cols]
        blocks.append(jnp.where(core == 0, own, other))
        blocks.append(jnp.where(core == 0, other, own))
    return jnp.concatenate(blocks, axis=0)


def project(core, x_ref, own_ref, other_ref, cols):
    acc = None
    for z in range(own_ref.shape[1] // 32):
        rhs = natural_rows(core, own_ref, other_ref, z, cols)
        part = jnp.dot(x_ref[:, 256 * z : 256 * z + 256], rhs, preferred_element_type=F32)
        acc = part if acc is None else acc + part
    return acc


def qkv_kernel(core_ref, x_ref, own_ref, other_ref, qg_ref, kg_ref, _, q_ref, kv_ref):
    acc = project(core_ref[0], x_ref, own_ref, other_ref, slice(0, own_ref.shape[2]))
    low = lax.broadcasted_iota(jnp.int32, (x_ref.shape[0], WIDTH), 1) < HEAD_DIM

    def normed(block, gain):
        squares = block * block
        first = jnp.sum(jnp.where(low, squares, 0.0), axis=1, keepdims=True)
        second = jnp.sum(jnp.where(low, 0.0, squares), axis=1, keepdims=True)
        first = lax.rsqrt(first / HEAD_DIM + EPS)
        second = lax.rsqrt(second / HEAD_DIM + EPS)
        return (block * jnp.where(low, first, second) * gain).astype(BF)

    tok, q_cols = x_ref.shape[0], q_ref.shape[2]
    for at in range(0, q_cols, WIDTH):
        q = normed(acc[:, at : at + WIDTH], qg_ref[...])
        for g in range(q_ref.shape[0]):
            q_ref[g, :tok, at : at + WIDTH] = q
    q_ref[:, tok:, :] = jnp.zeros((q_ref.shape[0], q_ref.shape[1] - tok, q_cols), BF)
    kv_ref[:, :WIDTH] = normed(acc[:, q_cols : q_cols + WIDTH], kg_ref[...])
    kv_ref[:, WIDTH:] = acc[:, q_cols + WIDTH :].astype(BF)


SMEM = pl.BlockSpec(memory_space=pltpu.SMEM)
VMEM = pl.BlockSpec(memory_space=pltpu.VMEM)


def qkv(core, x, own, other, query_gain, key_gain, packed):
    tok, q_cols = x.shape[0], own.shape[2] - 2 * WIDTH
    return pl.pallas_call(
        qkv_kernel,
        grid=(1,),
        in_specs=[SMEM] + [VMEM] * 5 + [pl.BlockSpec(memory_space=pl.ANY)],
        out_specs=[pl.BlockSpec((*packed.shape[:2], q_cols), lambda i: (0, 0, 0)), VMEM],
        out_shape=[
            jax.ShapeDtypeStruct(packed.shape, BF),
            jax.ShapeDtypeStruct((tok, 2 * WIDTH), BF),
        ],
        input_output_aliases={6: 0},
        name="qkv",
    )(core, x, own, other, jnp.tile(query_gain, 2)[None], jnp.tile(key_gain, 2)[None], packed)


def glu_kernel(
    core_ref, t_ref, x_ref, own_ref, other_ref, out_ref, head_ref, tail_ref, edge_ref, *, start
):
    n, seg, channels = out_ref.shape
    cols = slice(start, start + 2 * channels)
    acc = project(core_ref[0], x_ref, own_ref, other_ref, cols)
    value, gate = acc[:, :channels], acc[:, channels:]
    glu = value * (1.0 / (1.0 + jnp.exp(-gate)))
    for y in range(n):
        rows = glu[seg * y : seg * y + seg]
        out_ref[y] = rows.astype(BF)
        head_ref[y] = rows[:REACH].astype(BF)
        tail_ref[y] = rows[seg - REACH :].astype(BF)
    first, last = glu[:REACH], glu[n * seg - REACH :]
    edge_ref[0] = jnp.where(t_ref[0] == 0, first, last).astype(BF)


def glu_of(core, t, x, own, other, start, channels, n):
    reach = jax.ShapeDtypeStruct((n, REACH, channels), BF)
    return pl.pallas_call(
        functools.partial(glu_kernel, start=start),
        in_specs=[SMEM] * 2 + [VMEM] * 3,
        out_specs=[VMEM] * 4,
        out_shape=[
            jax.ShapeDtypeStruct((n, x.shape[0] // n, channels), BF),
            reach,
            reach,
            jax.ShapeDtypeStruct((1, REACH, channels), BF),
        ],
        name="glu",
    )(core, t, x, own, other)


def wide_eye(rows):
    eye = lax.broadcasted_iota(jnp.int32, (rows, WIDTH), 0)
    return eye == lax.broadcasted_iota(jnp.int32, (rows, WIDTH), 1)


def conv_kernel(
    t_ref, glu_ref, left_ref, right_ref, edge_ref, w_ref, sum_ref, sq_ref, pad_ref
):
    n, seg, _ = glu_ref.shape
    t = t_ref[0]
    for y in range(n):
        inner = edge_ref[0] if y == 0 else left_ref[y - 1]
        pad_ref[y, :REACH] = jnp.where(t == 0, inner, left_ref[y]).astype(F32)
        pad_ref[y, REACH : REACH + seg] = glu_ref[y].astype(F32)
        inner = edge_ref[0] if y == n - 1 else right_ref[y + 1]
        pad_ref[y, REACH + seg : 2 * REACH + seg] = jnp.where(
            t == n - 1, inner, right_ref[y]
        ).astype(F32)
    lines = []
    for y in range(n):
        acc = jnp.zeros((seg, glu_ref.shape[2]), F32)
        for j in range(CONV_W):
            acc = acc + w_ref[j : j + 1, :] * pad_ref[y, j : j + seg]
        sum_ref[y] = acc
        column = jnp.sum(acc * acc, axis=1, keepdims=True)
        lines.append(jnp.sum(jnp.where(wide_eye(seg), column, 0.0), axis=0, keepdims=True))
    lines = jnp.concatenate(lines, axis=0)
    for g in range(sq_ref.shape[0]):
        sq_ref[g] = lines


def conv_of(t, glu, left, right, edge, weight):
    n, seg, channels = glu.shape
    return pl.pallas_call(
        conv_kernel,
        in_specs=[SMEM] + [VMEM] * 5,
        out_specs=[VMEM, VMEM],
        out_shape=[
            jax.ShapeDtypeStruct((n, seg, channels), F32),
            jax.ShapeDtypeStruct((n, n, WIDTH), F32),
        ],
        scratch_shapes=[pltpu.VMEM((n, 64, channels), F32)],
        name="conv",
    )(t, glu, left, right, edge, weight)


def out_kernel(
    core_ref, att_ref, conv_ref, sq_ref, gain_ref, own_ref, other_ref, out_ref, act_ref, *, start
):
    n, seg, _ = out_ref.shape
    channels = conv_ref.shape[2]
    cols = slice(start, start + att_ref.shape[1] + channels)
    squares = sq_ref[0]
    for g in range(1, n):
        squares = squares + sq_ref[g]
    for y in range(n):
        line = jnp.broadcast_to(squares[y : y + 1], (seg, WIDTH))
        column = jnp.sum(jnp.where(wide_eye(seg), line, 0.0), axis=1, keepdims=True)
        scaled = conv_ref[y] * lax.rsqrt(column / C_CH + EPS) * gain_ref[...]
        act_ref[seg * y : seg * y + seg, :] = scaled * (1.0 / (1.0 + jnp.exp(-scaled)))
    act = jnp.concatenate([att_ref[...], act_ref[...].astype(BF)], axis=1)
    for z in range(own_ref.shape[1] // 32):
        rhs = natural_rows(core_ref[0], own_ref, other_ref, z, cols)
        term = contract_last(act, rhs)
        for y in range(n):
            block = term[seg * y : seg * y + seg]
            out_ref[y, :, 256 * z : 256 * z + 256] = block.astype(BF)


def out_of(core, att, conv, squares, gain, own, other, start):
    n, seg, channels = conv.shape
    width = own.shape[0] * own.shape[1] * 2
    return pl.pallas_call(
        functools.partial(out_kernel, start=start),
        in_specs=[SMEM] + [VMEM] * 6,
        out_specs=VMEM,
        out_shape=jax.ShapeDtypeStruct((n, seg, width), BF),
        scratch_shapes=[pltpu.VMEM((n * seg, channels), F32)],
        name="out",
    )(core, att, conv, squares, gain[None], own, other)


def local(
    tokens,
    norm_gain,
    query_weight,
    key_weight,
    value_weight,
    glu_value_weight,
    glu_gate_weight,
    query_gain,
    key_gain,
    lambdas,
    head_gain,
    conv_weight,
    channel_gain,
    attn_out_weight,
    conv_out_weight,
):
    n = lax.axis_size("y")
    heads = query_weight.shape[1] // WIDTH
    tok = tokens.shape[0]
    seg = tok // n
    channels = conv_weight.shape[1]

    row_of = [t // 2 + (n // 2) * (t % 2) for t in range(n)]
    swap = [(y * n + t, row_of[t] * n + y) for y in range(n) for t in range(n)]
    weights = (query_weight, key_weight, value_weight, glu_value_weight, glu_gate_weight)
    weights = weights + (attn_out_weight, conv_out_weight)
    first = sum(w.shape[1] for w in weights[:3])
    columns = sum(w.shape[1] for w in weights)
    shard = lax.ppermute(jnp.concatenate(weights, axis=1), PLANE, swap)
    small = jnp.concatenate(
        [
            conv_weight,
            channel_gain[None],
            jnp.pad(lambdas, (0, channels - heads))[None],
            jnp.zeros((7, channels), F32),
        ],
        axis=0,
    )
    small = lax.ppermute(small, PLANE, swap)
    lambdas = small[CONV_W + 1, :heads]

    blocks = tokens.reshape(n, seg, tokens.shape[1])
    blocks = jnp.broadcast_to(blocks, (n, *blocks.shape)).reshape(n * n, seg, -1)
    mine = lax.all_to_all(blocks, PLANE, 0, 0, tiled=True)
    mine = mine.reshape(n, n, seg, -1)
    gathered = mine.transpose(0, 2, 1, 3).reshape(n, seg, -1).astype(F32)
    normed = rms_scale(gathered, norm_gain).astype(BF).reshape(tok, -1)

    by_z = lax.all_gather(shard, "z", axis=0)
    core = lax.axis_index("c").astype(jnp.int32)[None]
    mates = [(0, 1), (1, 0)]
    by_z = by_z.reshape(-1, by_z.shape[2])
    wa = copies_to(by_z[:, :first], "x")
    wa_other = lax.ppermute(wa, "c", mates)
    fold = math.log2(math.e) * HEAD_DIM ** (-0.5)
    q_cols = query_weight.shape[1]
    late = columns - first
    rest = jnp.pad(by_z[:, first:], ((0, 0), (q_cols, -(q_cols + late) % WIDTH)))
    rest = jnp.broadcast_to(rest, (lax.axis_size("x"), *rest.shape))
    rest, kv = qkv(core, normed, wa, wa_other, query_gain * fold, key_gain, rest)
    rest = lax.all_to_all(rest, "x", 0, 0, tiled=True)
    kv = lax.all_gather(kv, "z", axis=0, tiled=True)
    kv_other = lax.ppermute(kv, "c", mates)
    rest_other = lax.ppermute(rest, "c", mates)
    parts = attend(rest, tok, q_cols, kv, kv_other, 1792, 896, 256)
    arrived = lax.all_to_all(parts, "x", 0, 0, tiled=True)
    att = combine(arrived, lambdas, head_gain, tok, heads)

    g_cols = glu_value_weight.shape[1]
    t = lax.axis_index(TP).astype(jnp.int32)[None]
    glu, heads_rows, tails, edge = glu_of(
        core, t, normed, rest, rest_other, q_cols, g_cols, n
    )
    size_z = lax.axis_size("z")
    ring = [(i, (i + 1) % n) for i in range(n)]
    left = lax.ppermute(tails, TP, ring)
    right = lax.ppermute(heads_rows, TP, [(b, a) for a, b in ring])
    across = [(z * n + n - 1, (z + 1) * n) for z in range(size_z - 1)]
    across = [(z * n + n - 1, (z + 1) * n) for z in range(size_z - 1)]
    across = across + [(b, a) for a, b in across]
    edge = lax.ppermute(edge, TOK_RING, across)
    conv_sum, squares = conv_of(t, glu, left, right, edge, small[:CONV_W])
    squares = lax.all_to_all(squares, "y", 0, 0, tiled=True)
    term = out_of(
        core, att, conv_sum, squares, small[CONV_W], rest, rest_other, q_cols + 2 * g_cols
    )
    reduced = lax.all_to_all(term, "y", 0, 0, tiled=True)
    return reduced.astype(F32).sum(axis=0).astype(BF)


def solution(mesh):
    finer = Mesh(mesh.devices.reshape(8, 8, 4, 2), ("z", "y", "x", "c"))
    sp = ("z", "y")
    both, rows = P(sp, TP), P()
    placed = (both, rows) + (both,) * 5 + (rows, rows, P(TP), rows, P(None, TP), P(TP), both, both)
    return jax.shard_map(
        local, mesh=finer, in_specs=placed, out_specs=P(sp + TP, None), check_vma=False
    )
```

```python
import functools
import math

import jax
import jax.numpy as jnp
from jax import lax
from jax.experimental import pallas as pl
from jax.experimental.pallas import tpu as pltpu
from jax.sharding import Mesh
from jax.sharding import PartitionSpec as P

HEAD_DIM = 64
WIDTH = 2 * HEAD_DIM
C_CH = 1536
CONV_W = 31
REACH = CONV_W // 2
EPS = 1e-06
LAMBDA_INIT = 0.2
BF = jnp.bfloat16
F32 = jnp.float32
TP = ("x", "c")
PLANE = ("y", "x", "c")
TOK_RING = ("z", "x", "c")
SMEM = pl.BlockSpec(memory_space=pltpu.SMEM)
VMEM = pl.BlockSpec(memory_space=pltpu.VMEM)


def rms_scale(values, gain):
    return values * lax.rsqrt(jnp.mean(values * values, axis=-1, keepdims=True) + EPS) * gain


def contract_last(left, right):
    return lax.dot_general(left, right, (((1,), (1,)), ((), ())), preferred_element_type=F32)


def copies_to(array, axis):
    copies = jnp.broadcast_to(array, (lax.axis_size(axis), *array.shape))
    return lax.all_to_all(copies, axis, 0, 0, tiled=True)


def diagonal(size):
    rows = lax.broadcasted_iota(jnp.int32, (size, size), 0)
    return rows == lax.broadcasted_iota(jnp.int32, (size, size), 1)


def pack_kernel(x_ref, out_ref):
    seg = out_ref.shape[1] // 2
    n = x_ref.shape[0] // seg
    for t in range(n):
        rows = x_ref[seg * t : seg * t + seg, :]
        for y in range(n):
            out_ref[n * y + t, :seg, :] = rows[:, :WIDTH]
            out_ref[n * y + t, seg:, :] = rows[:, WIDTH:]


def norm_kernel(x_ref, gain_ref, out_ref):
    n = out_ref.shape[1] // (2 * WIDTH)
    seg = x_ref.shape[1] // 2
    for y in range(out_ref.shape[0] // seg):
        blocks = []
        for t in range(n):
            block = x_ref[n * y + t].astype(F32)
            blocks += [block[:seg], block[seg:]]
        squares = blocks[0] * blocks[0]
        for block in blocks[1:]:
            squares = squares + block * block
        mean = jnp.sum(squares, axis=1, keepdims=True) / out_ref.shape[1]
        scale = lax.rsqrt(mean + EPS)
        for b, block in enumerate(blocks):
            cols = slice(WIDTH * b, WIDTH * b + WIDTH)
            normed = block * scale * gain_ref[:, cols]
            out_ref[seg * y : seg * y + seg, cols] = normed.astype(BF)


def pack(tokens, n):
    tok, _ = tokens.shape
    return pl.pallas_call(
        pack_kernel,
        in_specs=[VMEM],
        out_specs=VMEM,
        out_shape=jax.ShapeDtypeStruct((n * n, 2 * tok // n, WIDTH), BF),
        name="pack",
    )(tokens)


def norm_of(blocks, gain, n):
    return pl.pallas_call(
        norm_kernel,
        in_specs=[VMEM, VMEM],
        out_specs=VMEM,
        out_shape=jax.ShapeDtypeStruct((n * blocks.shape[1] // 2, gain.shape[0]), BF),
        name="norm",
    )(blocks, gain[None])


def attend_kernel(
    qs_ref, k0_ref, v0_ref, k1_ref, v1_ref, o_ref, acc_ref, q_ref, *, tok, rows, keys
):
    step = pl.program_id(0)

    @pl.when(step == 0)
    def _():
        acc_ref[...] = jnp.zeros_like(acc_ref)
        groups = qs_ref.shape[0]
        pair = lax.broadcasted_iota(jnp.int32, (tok, WIDTH), 1) // HEAD_DIM
        at = 0
        for g in range(groups):
            for h in range(qs_ref.shape[2] // WIDTH):
                q = qs_ref[g, :tok, h * WIDTH : (h + 1) * WIDTH].astype(F32)
                for p in range(2):
                    q_ref[at : at + tok, :] = jnp.where(pair == p, q, 0.0).astype(BF)
                    at += tok

    ones = jnp.ones((keys, WIDTH), BF)
    for k_ref, v_ref in ((k0_ref, v0_ref), (k1_ref, v1_ref)):
        for j in range(k_ref.shape[0] // keys):
            k = k_ref[j * keys : (j + 1) * keys, :]
            v = jnp.concatenate([v_ref[j * keys : (j + 1) * keys, :], ones], axis=1)
            for r in range(q_ref.shape[0] // rows):
                part = pl.ds(r * rows, rows)
                s = contract_last(q_ref[part, :], k)
                e = jnp.exp2(s).astype(BF)
                acc_ref[part, :] += jnp.dot(e, v, preferred_element_type=F32)

    @pl.when(step == pl.num_programs(0) - 1)
    def _():
        groups, padded, _ = o_ref.shape
        count = acc_ref.shape[0] // groups
        eye = diagonal(WIDTH)
        for g in range(groups):
            o_ref[g, :count, :] = acc_ref[g * count : (g + 1) * count, :WIDTH].astype(BF)
            lines = []
            for j in range(count // WIDTH):
                start = g * count + j * WIDTH
                block = acc_ref[start : start + WIDTH, WIDTH:]
                lines.append(jnp.sum(jnp.where(eye, block, 0.0), axis=0, keepdims=True))
            lines.append(jnp.zeros((8 - len(lines), WIDTH), F32))
            sums = jnp.concatenate(lines, axis=0)
            high = sums.astype(BF).astype(F32)
            both = jnp.concatenate([high, sums - high], axis=0)
            o_ref[g, count:padded, :] = both.astype(BF)


def attend(packed, tok, cols, kv_own, kv_other, block, rows, keys):
    groups = packed.shape[0]
    each, total = 2 * tok * (cols // WIDTH), kv_own.shape[0]
    count = groups * each
    half = [pl.BlockSpec((block, WIDTH), lambda i, h=h: (i, h)) for h in (0, 1)]
    return pl.pallas_call(
        functools.partial(attend_kernel, tok=tok, rows=rows, keys=keys),
        grid=(total // block,),
        in_specs=[pl.BlockSpec((groups, packed.shape[1], cols), lambda i: (0, 0, 2))] + half + half,
        out_specs=pl.BlockSpec((groups, each + 16, WIDTH), lambda i: (0, 0, 0)),
        out_shape=jax.ShapeDtypeStruct((groups, each + 16, WIDTH), BF),
        scratch_shapes=[pltpu.VMEM((count, 2 * WIDTH), F32), pltpu.VMEM((count, WIDTH), BF)],
        cost_estimate=pl.CostEstimate(
            flops=12 * count * total * WIDTH,
            transcendentals=2 * count * total,
            bytes_accessed=total * 8 * WIDTH + count * 4 * WIDTH,
        ),
        name="attend",
    )(packed, kv_own, kv_own, kv_other, kv_other)


def combine_kernel(parts_ref, lam_ref, gain_ref, out_ref, ratio_ref):
    count = parts_ref.shape[1] - 16
    total = parts_ref[0].astype(F32)
    for g in range(1, parts_ref.shape[0]):
        total = total + parts_ref[g].astype(F32)
    sums = total[count : count + 8] + total[count + 8 : count + 16]
    eye = diagonal(WIDTH)
    for j in range(count // WIDTH):
        line = jnp.broadcast_to(sums[j : j + 1], (WIDTH, WIDTH))
        column = jnp.sum(jnp.where(eye, line, 0.0), axis=1, keepdims=True)
        ratio_ref[j * WIDTH : (j + 1) * WIDTH, :] = total[j * WIDTH : (j + 1) * WIDTH] / column
    tok = out_ref.shape[0]
    for h in range(out_ref.shape[1] // WIDTH):
        start = 2 * h * tok
        first = ratio_ref[start : start + tok, :]
        second = ratio_ref[start + tok : start + 2 * tok, :]
        o = first - lam_ref[h : h + 1, :] * second
        o = rms_scale(o, gain_ref[...]) * (1.0 - LAMBDA_INIT)
        out_ref[:, h * WIDTH : (h + 1) * WIDTH] = o.astype(BF)


def combine(parts, lam, gain, tok, heads):
    count = parts.shape[1] - 16
    lam_rows = jnp.broadcast_to(jnp.pad(lam, (0, 8 - heads))[:, None], (8, WIDTH))
    return pl.pallas_call(
        combine_kernel,
        out_shape=jax.ShapeDtypeStruct((tok, heads * WIDTH), BF),
        scratch_shapes=[pltpu.VMEM((count, WIDTH), F32)],
        name="combine",
    )(parts, lam_rows, gain.reshape(1, WIDTH))


def natural_rows(core, own_ref, other_ref, z, cols):
    blocks = []
    for x in range(own_ref.shape[0]):
        own = own_ref[x, 32 * z : 32 * z + 32, cols]
        other = other_ref[x, 32 * z : 32 * z + 32, cols]
        blocks.append(jnp.where(core == 0, own, other))
        blocks.append(jnp.where(core == 0, other, own))
    return jnp.concatenate(blocks, axis=0)


def project(core, x_ref, own_ref, other_ref, cols):
    acc = None
    for z in range(own_ref.shape[1] // 32):
        rhs = natural_rows(core, own_ref, other_ref, z, cols)
        part = jnp.dot(x_ref[:, 256 * z : 256 * z + 256], rhs, preferred_element_type=F32)
        acc = part if acc is None else acc + part
    return acc


def qkv_kernel(core_ref, x_ref, own_ref, other_ref, qg_ref, kg_ref, _, q_ref, kv_ref):
    acc = project(core_ref[0], x_ref, own_ref, other_ref, slice(0, own_ref.shape[2]))
    low = lax.broadcasted_iota(jnp.int32, (x_ref.shape[0], WIDTH), 1) < HEAD_DIM

    def normed(block, gain):
        squares = block * block
        first = jnp.sum(jnp.where(low, squares, 0.0), axis=1, keepdims=True)
        second = jnp.sum(jnp.where(low, 0.0, squares), axis=1, keepdims=True)
        first = lax.rsqrt(first / HEAD_DIM + EPS)
        second = lax.rsqrt(second / HEAD_DIM + EPS)
        return (block * jnp.where(low, first, second) * gain).astype(BF)

    tok, q_cols = x_ref.shape[0], q_ref.shape[2]
    for at in range(0, q_cols, WIDTH):
        q = normed(acc[:, at : at + WIDTH], qg_ref[...])
        for g in range(q_ref.shape[0]):
            q_ref[g, :tok, at : at + WIDTH] = q
    q_ref[:, tok:, :] = jnp.zeros((q_ref.shape[0], q_ref.shape[1] - tok, q_cols), BF)
    kv_ref[:, :WIDTH] = normed(acc[:, q_cols : q_cols + WIDTH], kg_ref[...])
    kv_ref[:, WIDTH:] = acc[:, q_cols + WIDTH :].astype(BF)


def qkv(core, x, own, other, query_gain, key_gain, packed):
    tok, q_cols = x.shape[0], own.shape[2] - 2 * WIDTH
    return pl.pallas_call(
        qkv_kernel,
        grid=(1,),
        in_specs=[SMEM] + [VMEM] * 5 + [pl.BlockSpec(memory_space=pl.ANY)],
        out_specs=[pl.BlockSpec((*packed.shape[:2], q_cols), lambda i: (0, 0, 2)), VMEM],
        out_shape=[
            jax.ShapeDtypeStruct(packed.shape, BF),
            jax.ShapeDtypeStruct((tok, 2 * WIDTH), BF),
        ],
        input_output_aliases={6: 0},
        name="qkv",
    )(core, x, own, other, jnp.tile(query_gain, 2)[None], jnp.tile(key_gain, 2)[None], packed)


def glu_kernel(
    core_ref, t_ref, x_ref, own_ref, other_ref, out_ref, head_ref, tail_ref, edge_ref
):
    n, seg, channels = out_ref.shape
    cols = slice(0, 2 * channels)
    acc = project(core_ref[0], x_ref, own_ref, other_ref, cols)
    value, gate = acc[:, :channels], acc[:, channels:]
    glu = value * (1.0 / (1.0 + jnp.exp(-gate)))
    for y in range(n):
        rows = glu[seg * y : seg * y + seg]
        out_ref[y] = rows.astype(BF)
        head_ref[y] = rows[:REACH].astype(BF)
        tail_ref[y] = rows[seg - REACH :].astype(BF)
    first, last = glu[:REACH], glu[n * seg - REACH :]
    edge_ref[0] = jnp.where(t_ref[0] == 0, first, last).astype(BF)


def glu_of(core, t, x, own, other, channels, n):
    reach = jax.ShapeDtypeStruct((n, REACH, channels), BF)
    return pl.pallas_call(
        glu_kernel,
        grid=(1,),
        in_specs=[SMEM] * 2
        + [VMEM]
        + [pl.BlockSpec((*own.shape[:2], 2 * channels), lambda i: (0, 0, 2))] * 2,
        out_specs=[VMEM] * 4,
        out_shape=[
            jax.ShapeDtypeStruct((n, x.shape[0] // n, channels), BF),
            reach,
            reach,
            jax.ShapeDtypeStruct((1, REACH, channels), BF),
        ],
        name="glu",
    )(core, t, x, own, other)


def wide_eye(rows):
    eye = lax.broadcasted_iota(jnp.int32, (rows, WIDTH), 0)
    return eye == lax.broadcasted_iota(jnp.int32, (rows, WIDTH), 1)


def conv_kernel(
    t_ref, glu_ref, left_ref, right_ref, edge_ref, w_ref, sum_ref, sq_ref, pad_ref
):
    n, seg, _ = glu_ref.shape
    t = t_ref[0]
    for y in range(n):
        inner = edge_ref[0] if y == 0 else left_ref[y - 1]
        pad_ref[y, :REACH] = jnp.where(t == 0, inner, left_ref[y]).astype(F32)
        pad_ref[y, REACH : REACH + seg] = glu_ref[y].astype(F32)
        inner = edge_ref[0] if y == n - 1 else right_ref[y + 1]
        pad_ref[y, REACH + seg : 2 * REACH + seg] = jnp.where(
            t == n - 1, inner, right_ref[y]
        ).astype(F32)
    lines = []
    for y in range(n):
        acc = jnp.zeros((seg, glu_ref.shape[2]), F32)
        for j in range(CONV_W):
            acc = acc + w_ref[j : j + 1, :] * pad_ref[y, j : j + seg]
        sum_ref[y] = acc
        column = jnp.sum(acc * acc, axis=1, keepdims=True)
        lines.append(jnp.sum(jnp.where(wide_eye(seg), column, 0.0), axis=0, keepdims=True))
    lines = jnp.concatenate(lines, axis=0)
    for g in range(sq_ref.shape[0]):
        sq_ref[g] = lines


def conv_of(t, glu, left, right, edge, weight):
    n, seg, channels = glu.shape
    return pl.pallas_call(
        conv_kernel,
        in_specs=[SMEM] + [VMEM] * 5,
        out_specs=[VMEM, VMEM],
        out_shape=[
            jax.ShapeDtypeStruct((n, seg, channels), F32),
            jax.ShapeDtypeStruct((n, n, WIDTH), F32),
        ],
        scratch_shapes=[pltpu.VMEM((n, 64, channels), F32)],
        name="conv",
    )(t, glu, left, right, edge, weight)


def out_kernel(
    core_ref, att_ref, conv_ref, sq_ref, gain_ref, own_ref, other_ref, out_ref, act_ref
):
    n, seg, channels = conv_ref.shape
    cols = slice(0, att_ref.shape[1] + channels)
    squares = sq_ref[0]
    for g in range(1, n):
        squares = squares + sq_ref[g]
    for y in range(n):
        line = jnp.broadcast_to(squares[y : y + 1], (seg, WIDTH))
        column = jnp.sum(jnp.where(wide_eye(seg), line, 0.0), axis=1, keepdims=True)
        scaled = conv_ref[y] * lax.rsqrt(column / C_CH + EPS) * gain_ref[...]
        act_ref[seg * y : seg * y + seg, :] = scaled * (1.0 / (1.0 + jnp.exp(-scaled)))
    act = jnp.concatenate([att_ref[...], act_ref[...].astype(BF)], axis=1)
    for z in range(own_ref.shape[1] // 32):
        rhs = natural_rows(core_ref[0], own_ref, other_ref, z, cols)
        term = contract_last(act, rhs)
        for y in range(n):
            block = term[seg * y : seg * y + seg].astype(BF)
            at = 2 * z * seg
            out_ref[y, at : at + seg, :] = block[:, :WIDTH]
            out_ref[y, at + seg : at + 2 * seg, :] = block[:, WIDTH:]


def out_of(core, att, conv, squares, gain, own, other, pad):
    n, seg, channels = conv.shape
    width = own.shape[0] * own.shape[1] * 2
    late = (*own.shape[:2], att.shape[1] + channels + pad)
    return pl.pallas_call(
        out_kernel,
        grid=(1,),
        in_specs=[SMEM] + [VMEM] * 4 + [pl.BlockSpec(late, lambda i: (0, 0, 0))] * 2,
        out_specs=VMEM,
        out_shape=jax.ShapeDtypeStruct((n, seg * width // WIDTH, WIDTH), BF),
        scratch_shapes=[pltpu.VMEM((n * seg, channels), F32)],
        name="out",
    )(core, att, conv, squares, gain[None], own, other)


def sum_kernel(x_ref, out_ref):
    seg = out_ref.shape[0]
    for b in range(out_ref.shape[1] // WIDTH):
        total = x_ref[0, seg * b : seg * b + seg, :].astype(F32)
        for g in range(1, x_ref.shape[0]):
            total = total + x_ref[g, seg * b : seg * b + seg, :].astype(F32)
        out_ref[:, WIDTH * b : WIDTH * b + WIDTH] = total.astype(BF)


def sum_of(parts, seg):
    return pl.pallas_call(
        sum_kernel,
        in_specs=[VMEM],
        out_specs=VMEM,
        out_shape=jax.ShapeDtypeStruct((seg, parts.shape[1] // seg * WIDTH), BF),
        name="sum",
    )(parts)


def local(
    tokens,
    norm_gain,
    query_weight,
    key_weight,
    value_weight,
    glu_value_weight,
    glu_gate_weight,
    query_gain,
    key_gain,
    lambdas,
    head_gain,
    conv_weight,
    channel_gain,
    attn_out_weight,
    conv_out_weight,
):
    n = lax.axis_size("y")
    heads = query_weight.shape[1] // WIDTH
    tok = tokens.shape[0]
    seg = tok // n
    channels = conv_weight.shape[1]

    row_of = [t // 2 + (n // 2) * (t % 2) for t in range(n)]
    swap = [(y * n + t, row_of[t] * n + y) for y in range(n) for t in range(n)]
    weights = (query_weight, key_weight, value_weight, glu_value_weight, glu_gate_weight)
    weights = weights + (attn_out_weight, conv_out_weight)
    first = sum(w.shape[1] for w in weights[:3])
    columns = sum(w.shape[1] for w in weights)
    shard = lax.ppermute(jnp.concatenate(weights, axis=1), PLANE, swap)
    small = jnp.concatenate(
        [
            conv_weight,
            channel_gain[None],
            jnp.pad(lambdas, (0, channels - heads))[None],
            jnp.zeros((7, channels), F32),
        ],
        axis=0,
    )
    small = lax.ppermute(small, PLANE, swap)
    lambdas = small[CONV_W + 1, :heads]

    blocks = pack(tokens, n)
    mine = lax.all_to_all(blocks, PLANE, 0, 0, tiled=True)
    normed = norm_of(mine, norm_gain, n)

    by_z = lax.all_gather(shard, "z", axis=0)
    core = lax.axis_index("c").astype(jnp.int32)[None]
    mates = [(0, 1), (1, 0)]
    by_z = by_z.reshape(-1, by_z.shape[2])
    wa = copies_to(by_z[:, :first], "x")
    wa_other = lax.ppermute(wa, "c", mates)
    fold = math.log2(math.e) * HEAD_DIM ** (-0.5)
    q_cols = query_weight.shape[1]
    g_cols = glu_value_weight.shape[1]
    late = first + 2 * g_cols
    pad = -(columns - late) % q_cols
    gap = jnp.zeros((by_z.shape[0], pad + q_cols), BF)
    rest = jnp.concatenate([by_z[:, late:], gap, by_z[:, first:late]], axis=1)
    rest = jnp.broadcast_to(rest, (lax.axis_size("x"), *rest.shape))
    rest, kv = qkv(core, normed, wa, wa_other, query_gain * fold, key_gain, rest)
    rest = lax.all_to_all(rest, "x", 0, 0, tiled=True)
    kv = lax.all_gather(kv, "z", axis=0, tiled=True)
    kv_other = lax.ppermute(kv, "c", mates)
    rest_other = lax.ppermute(rest, "c", mates)
    parts = attend(rest, tok, q_cols, kv, kv_other, 1792, 896, 256)
    arrived = lax.all_to_all(parts, "x", 0, 0, tiled=True)
    att = combine(arrived, lambdas, head_gain, tok, heads)

    t = lax.axis_index(TP).astype(jnp.int32)[None]
    glu, heads_rows, tails, edge = glu_of(
        core, t, normed, rest, rest_other, g_cols, n
    )
    size_z = lax.axis_size("z")
    ring = [(i, (i + 1) % n) for i in range(n)]
    left = lax.ppermute(tails, TP, ring)
    right = lax.ppermute(heads_rows, TP, [(b, a) for a, b in ring])
    across = [(z * n + n - 1, (z + 1) * n) for z in range(size_z - 1)]
    across = [(z * n + n - 1, (z + 1) * n) for z in range(size_z - 1)]
    across = across + [(b, a) for a, b in across]
    edge = lax.ppermute(edge, TOK_RING, across)
    conv_sum, squares = conv_of(t, glu, left, right, edge, small[:CONV_W])
    squares = lax.all_to_all(squares, "y", 0, 0, tiled=True)
    term = out_of(
        core, att, conv_sum, squares, small[CONV_W], rest, rest_other, pad
    )
    reduced = lax.all_to_all(term, "y", 0, 0, tiled=True)
    return sum_of(reduced, seg)


def solution(mesh):
    finer = Mesh(mesh.devices.reshape(8, 8, 4, 2), ("z", "y", "x", "c"))
    sp = ("z", "y")
    both, rows = P(sp, TP), P()
    placed = (both, rows) + (both,) * 5 + (rows, rows, P(TP), rows, P(None, TP), P(TP), both, both)
    return jax.shard_map(
        local, mesh=finer, in_specs=placed, out_specs=P(sp + TP, None), check_vma=False
    )
```

```python
import functools
import math

import jax
import jax.numpy as jnp
from jax import lax
from jax.experimental import pallas as pl
from jax.experimental.pallas import tpu as pltpu
from jax.sharding import Mesh
from jax.sharding import PartitionSpec as P

HEAD_DIM = 64
WIDTH = 2 * HEAD_DIM
C_CH = 1536
CONV_W = 31
REACH = CONV_W // 2
EPS = 1e-06
LAMBDA_INIT = 0.2
BF = jnp.bfloat16
F32 = jnp.float32
TP = ("x", "c")
PLANE = ("y", "x", "c")
TOK_RING = ("z", "x", "c")
SMEM = pl.BlockSpec(memory_space=pltpu.SMEM)
VMEM = pl.BlockSpec(memory_space=pltpu.VMEM)


def rms_scale(values, gain):
    return values * lax.rsqrt(jnp.mean(values * values, axis=-1, keepdims=True) + EPS) * gain


def contract_last(left, right):
    return lax.dot_general(left, right, (((1,), (1,)), ((), ())), preferred_element_type=F32)


def copies_to(array, axis):
    copies = jnp.broadcast_to(array, (lax.axis_size(axis), *array.shape))
    return lax.all_to_all(copies, axis, 0, 0, tiled=True)


def diagonal(size):
    rows = lax.broadcasted_iota(jnp.int32, (size, size), 0)
    return rows == lax.broadcasted_iota(jnp.int32, (size, size), 1)


def pack_kernel(x_ref, out_ref):
    seg = out_ref.shape[1] // 2
    n = x_ref.shape[0] // seg
    for t in range(n):
        rows = x_ref[seg * t : seg * t + seg, :]
        for y in range(n):
            out_ref[n * y + t, :seg, :] = rows[:, :WIDTH]
            out_ref[n * y + t, seg:, :] = rows[:, WIDTH:]


def norm_kernel(x_ref, gain_ref, out_ref):
    n = out_ref.shape[1] // (2 * WIDTH)
    seg = x_ref.shape[1] // 2
    for y in range(out_ref.shape[0] // seg):
        blocks = []
        for t in range(n):
            block = x_ref[n * y + t].astype(F32)
            blocks += [block[:seg], block[seg:]]
        squares = blocks[0] * blocks[0]
        for block in blocks[1:]:
            squares = squares + block * block
        mean = jnp.sum(squares, axis=1, keepdims=True) / out_ref.shape[1]
        scale = lax.rsqrt(mean + EPS)
        for b, block in enumerate(blocks):
            cols = slice(WIDTH * b, WIDTH * b + WIDTH)
            normed = block * scale * gain_ref[:, cols]
            out_ref[seg * y : seg * y + seg, cols] = normed.astype(BF)


def pack(tokens, n):
    tok, _ = tokens.shape
    return pl.pallas_call(
        pack_kernel,
        in_specs=[VMEM],
        out_specs=VMEM,
        out_shape=jax.ShapeDtypeStruct((n * n, 2 * tok // n, WIDTH), BF),
        name="pack",
    )(tokens)


def norm_of(blocks, gain, n):
    return pl.pallas_call(
        norm_kernel,
        in_specs=[VMEM, VMEM],
        out_specs=VMEM,
        out_shape=jax.ShapeDtypeStruct((n * blocks.shape[1] // 2, gain.shape[0]), BF),
        name="norm",
    )(blocks, gain[None])


def attend_kernel(
    qs_ref, k0_ref, v0_ref, k1_ref, v1_ref, o_ref, acc_ref, q_ref, *, tok, rows, keys
):
    step = pl.program_id(0)

    @pl.when(step == 0)
    def _():
        acc_ref[...] = jnp.zeros_like(acc_ref)
        groups = qs_ref.shape[0]
        pair = lax.broadcasted_iota(jnp.int32, (tok, WIDTH), 1) // HEAD_DIM
        at = 0
        for g in range(groups):
            for h in range(qs_ref.shape[2] // WIDTH):
                q = qs_ref[g, :tok, h * WIDTH : (h + 1) * WIDTH].astype(F32)
                for p in range(2):
                    q_ref[at : at + tok, :] = jnp.where(pair == p, q, 0.0).astype(BF)
                    at += tok

    ones = jnp.ones((keys, WIDTH), BF)
    for k_ref, v_ref in ((k0_ref, v0_ref), (k1_ref, v1_ref)):
        for j in range(k_ref.shape[0] // keys):
            k = k_ref[j * keys : (j + 1) * keys, :]
            v = jnp.concatenate([v_ref[j * keys : (j + 1) * keys, :], ones], axis=1)
            for r in range(q_ref.shape[0] // rows):
                part = pl.ds(r * rows, rows)
                s = contract_last(q_ref[part, :], k)
                e = jnp.exp2(s).astype(BF)
                acc_ref[part, :] += jnp.dot(e, v, preferred_element_type=F32)

    @pl.when(step == pl.num_programs(0) - 1)
    def _():
        groups, padded, _ = o_ref.shape
        count = acc_ref.shape[0] // groups
        eye = diagonal(WIDTH)
        for g in range(groups):
            o_ref[g, :count, :] = acc_ref[g * count : (g + 1) * count, :WIDTH].astype(BF)
            lines = []
            for j in range(count // WIDTH):
                start = g * count + j * WIDTH
                block = acc_ref[start : start + WIDTH, WIDTH:]
                lines.append(jnp.sum(jnp.where(eye, block, 0.0), axis=0, keepdims=True))
            lines.append(jnp.zeros((8 - len(lines), WIDTH), F32))
            sums = jnp.concatenate(lines, axis=0)
            high = sums.astype(BF).astype(F32)
            both = jnp.concatenate([high, sums - high], axis=0)
            o_ref[g, count:padded, :] = both.astype(BF)


def attend(packed, tok, cols, kv_own, kv_other, block, rows, keys):
    groups = packed.shape[0]
    each, total = 2 * tok * (cols // WIDTH), kv_own.shape[0]
    count = groups * each
    half = [pl.BlockSpec((block, WIDTH), lambda i, h=h: (i, h)) for h in (0, 1)]
    return pl.pallas_call(
        functools.partial(attend_kernel, tok=tok, rows=rows, keys=keys),
        grid=(total // block,),
        in_specs=[pl.BlockSpec((groups, packed.shape[1], cols), lambda i: (0, 0, 2))] + half + half,
        out_specs=pl.BlockSpec((groups, each + 16, WIDTH), lambda i: (0, 0, 0)),
        out_shape=jax.ShapeDtypeStruct((groups, each + 16, WIDTH), BF),
        scratch_shapes=[pltpu.VMEM((count, 2 * WIDTH), F32), pltpu.VMEM((count, WIDTH), BF)],
        cost_estimate=pl.CostEstimate(
            flops=12 * count * total * WIDTH,
            transcendentals=2 * count * total,
            bytes_accessed=total * 8 * WIDTH + count * 4 * WIDTH,
        ),
        name="attend",
    )(packed, kv_own, kv_own, kv_other, kv_other)


def combine_kernel(parts_ref, lam_ref, gain_ref, out_ref, ratio_ref):
    count = parts_ref.shape[1] - 16
    total = parts_ref[0].astype(F32)
    for g in range(1, parts_ref.shape[0]):
        total = total + parts_ref[g].astype(F32)
    sums = total[count : count + 8] + total[count + 8 : count + 16]
    eye = diagonal(WIDTH)
    for j in range(count // WIDTH):
        line = jnp.broadcast_to(sums[j : j + 1], (WIDTH, WIDTH))
        column = jnp.sum(jnp.where(eye, line, 0.0), axis=1, keepdims=True)
        ratio_ref[j * WIDTH : (j + 1) * WIDTH, :] = total[j * WIDTH : (j + 1) * WIDTH] / column
    tok = out_ref.shape[0]
    for h in range(out_ref.shape[1] // WIDTH):
        start = 2 * h * tok
        first = ratio_ref[start : start + tok, :]
        second = ratio_ref[start + tok : start + 2 * tok, :]
        o = first - lam_ref[h : h + 1, :] * second
        o = rms_scale(o, gain_ref[...]) * (1.0 - LAMBDA_INIT)
        out_ref[:, h * WIDTH : (h + 1) * WIDTH] = o.astype(BF)


def combine(parts, lam, gain, tok, heads):
    count = parts.shape[1] - 16
    lam_rows = jnp.broadcast_to(jnp.pad(lam, (0, 8 - heads))[:, None], (8, WIDTH))
    return pl.pallas_call(
        combine_kernel,
        out_shape=jax.ShapeDtypeStruct((tok, heads * WIDTH), BF),
        scratch_shapes=[pltpu.VMEM((count, WIDTH), F32)],
        name="combine",
    )(parts, lam_rows, gain.reshape(1, WIDTH))


def natural_rows(core, own_ref, other_ref, z, cols):
    blocks = []
    for x in range(own_ref.shape[0]):
        own = own_ref[x, 32 * z : 32 * z + 32, cols]
        other = other_ref[x, 32 * z : 32 * z + 32, cols]
        blocks.append(jnp.where(core == 0, own, other))
        blocks.append(jnp.where(core == 0, other, own))
    return jnp.concatenate(blocks, axis=0)


def project(core, x_ref, own_ref, other_ref, cols):
    acc = None
    for z in range(own_ref.shape[1] // 32):
        rhs = natural_rows(core, own_ref, other_ref, z, cols)
        part = jnp.dot(x_ref[:, 256 * z : 256 * z + 256], rhs, preferred_element_type=F32)
        acc = part if acc is None else acc + part
    return acc


def qkv_kernel(core_ref, x_ref, own_ref, other_ref, qg_ref, kg_ref, _, q_ref, kv_ref):
    acc = project(core_ref[0], x_ref, own_ref, other_ref, slice(0, own_ref.shape[2]))
    low = lax.broadcasted_iota(jnp.int32, (x_ref.shape[0], WIDTH), 1) < HEAD_DIM

    def normed(block, gain):
        squares = block * block
        first = jnp.sum(jnp.where(low, squares, 0.0), axis=1, keepdims=True)
        second = jnp.sum(jnp.where(low, 0.0, squares), axis=1, keepdims=True)
        first = lax.rsqrt(first / HEAD_DIM + EPS)
        second = lax.rsqrt(second / HEAD_DIM + EPS)
        return (block * jnp.where(low, first, second) * gain).astype(BF)

    tok, q_cols = x_ref.shape[0], q_ref.shape[2]
    for at in range(0, q_cols, WIDTH):
        q = normed(acc[:, at : at + WIDTH], qg_ref[...])
        for g in range(q_ref.shape[0]):
            q_ref[g, :tok, at : at + WIDTH] = q
    q_ref[:, tok:, :] = jnp.zeros((q_ref.shape[0], q_ref.shape[1] - tok, q_cols), BF)
    kv_ref[:, :WIDTH] = normed(acc[:, q_cols : q_cols + WIDTH], kg_ref[...])
    kv_ref[:, WIDTH:] = acc[:, q_cols + WIDTH :].astype(BF)


def qkv(core, x, own, other, query_gain, key_gain, packed):
    tok, q_cols = x.shape[0], own.shape[2] - 2 * WIDTH
    return pl.pallas_call(
        qkv_kernel,
        grid=(1,),
        in_specs=[SMEM] + [VMEM] * 5 + [pl.BlockSpec(memory_space=pl.ANY)],
        out_specs=[pl.BlockSpec((*packed.shape[:2], q_cols), lambda i: (0, 0, 2)), VMEM],
        out_shape=[
            jax.ShapeDtypeStruct(packed.shape, BF),
            jax.ShapeDtypeStruct((tok, 2 * WIDTH), BF),
        ],
        input_output_aliases={6: 0},
        name="qkv",
    )(core, x, own, other, jnp.tile(query_gain, 2)[None], jnp.tile(key_gain, 2)[None], packed)


def glu_kernel(
    core_ref, t_ref, x_ref, own_ref, other_ref, out_ref, head_ref, tail_ref, edge_ref
):
    n, seg, channels = out_ref.shape
    cols = slice(0, 2 * channels)
    acc = project(core_ref[0], x_ref, own_ref, other_ref, cols)
    value, gate = acc[:, :channels], acc[:, channels:]
    glu = value * (1.0 / (1.0 + jnp.exp(-gate)))
    for y in range(n):
        rows = glu[seg * y : seg * y + seg]
        out_ref[y] = rows.astype(BF)
        head_ref[y] = rows[:REACH].astype(BF)
        tail_ref[y] = rows[seg - REACH :].astype(BF)
    first, last = glu[:REACH], glu[n * seg - REACH :]
    edge_ref[0] = jnp.where(t_ref[0] == 0, first, last).astype(BF)


def glu_of(core, t, x, own, other, channels, n):
    reach = jax.ShapeDtypeStruct((n, REACH, channels), BF)
    return pl.pallas_call(
        glu_kernel,
        grid=(1,),
        in_specs=[SMEM] * 2
        + [VMEM]
        + [pl.BlockSpec((*own.shape[:2], 2 * channels), lambda i: (0, 0, 2))] * 2,
        out_specs=[VMEM] * 4,
        out_shape=[
            jax.ShapeDtypeStruct((n, x.shape[0] // n, channels), BF),
            reach,
            reach,
            jax.ShapeDtypeStruct((1, REACH, channels), BF),
        ],
        name="glu",
    )(core, t, x, own, other)


def wide_eye(rows):
    eye = lax.broadcasted_iota(jnp.int32, (rows, WIDTH), 0)
    return eye == lax.broadcasted_iota(jnp.int32, (rows, WIDTH), 1)


def conv_kernel(
    t_ref, glu_ref, left_ref, right_ref, edge_ref, w_ref, sum_ref, sq_ref, pad_ref
):
    n, seg, _ = glu_ref.shape
    t = t_ref[0]
    for y in range(n):
        inner = edge_ref[0] if y == 0 else left_ref[y - 1]
        pad_ref[y, :REACH] = jnp.where(t == 0, inner, left_ref[y]).astype(F32)
        pad_ref[y, REACH : REACH + seg] = glu_ref[y].astype(F32)
        inner = edge_ref[0] if y == n - 1 else right_ref[y + 1]
        pad_ref[y, REACH + seg : 2 * REACH + seg] = jnp.where(
            t == n - 1, inner, right_ref[y]
        ).astype(F32)
    lines = []
    for y in range(n):
        acc = jnp.zeros((seg, glu_ref.shape[2]), F32)
        for r in range(8):
            taps = range(r, CONV_W, 8)
            shifted = pad_ref[y, r : taps[-1] + seg]
            for j in taps:
                acc = acc + w_ref[j : j + 1, :] * shifted[j - r : j - r + seg]
        sum_ref[y] = acc
        column = jnp.sum(acc * acc, axis=1, keepdims=True)
        lines.append(jnp.sum(jnp.where(wide_eye(seg), column, 0.0), axis=0, keepdims=True))
    lines = jnp.concatenate(lines, axis=0)
    for g in range(sq_ref.shape[0]):
        sq_ref[g] = lines


def conv_of(t, glu, left, right, edge, weight):
    n, seg, channels = glu.shape
    return pl.pallas_call(
        conv_kernel,
        in_specs=[SMEM] + [VMEM] * 5,
        out_specs=[VMEM, VMEM],
        out_shape=[
            jax.ShapeDtypeStruct((n, seg, channels), F32),
            jax.ShapeDtypeStruct((n, n, WIDTH), F32),
        ],
        scratch_shapes=[pltpu.VMEM((n, 64, channels), F32)],
        name="conv",
    )(t, glu, left, right, edge, weight)


def out_kernel(
    core_ref, att_ref, conv_ref, sq_ref, gain_ref, own_ref, other_ref, out_ref, act_ref
):
    n, seg, channels = conv_ref.shape
    cols = slice(0, att_ref.shape[1] + channels)
    squares = sq_ref[0]
    for g in range(1, n):
        squares = squares + sq_ref[g]
    for y in range(n):
        line = jnp.broadcast_to(squares[y : y + 1], (seg, WIDTH))
        column = jnp.sum(jnp.where(wide_eye(seg), line, 0.0), axis=1, keepdims=True)
        scaled = conv_ref[y] * lax.rsqrt(column / C_CH + EPS) * gain_ref[...]
        act_ref[seg * y : seg * y + seg, :] = scaled * (1.0 / (1.0 + jnp.exp(-scaled)))
    act = jnp.concatenate([att_ref[...], act_ref[...].astype(BF)], axis=1)
    for z in range(own_ref.shape[1] // 32):
        rhs = natural_rows(core_ref[0], own_ref, other_ref, z, cols)
        term = contract_last(act, rhs)
        for y in range(n):
            block = term[seg * y : seg * y + seg].astype(BF)
            at = 2 * z * seg
            out_ref[y, at : at + seg, :] = block[:, :WIDTH]
            out_ref[y, at + seg : at + 2 * seg, :] = block[:, WIDTH:]


def out_of(core, att, conv, squares, gain, own, other, pad):
    n, seg, channels = conv.shape
    width = own.shape[0] * own.shape[1] * 2
    late = (*own.shape[:2], att.shape[1] + channels + pad)
    return pl.pallas_call(
        out_kernel,
        grid=(1,),
        in_specs=[SMEM] + [VMEM] * 4 + [pl.BlockSpec(late, lambda i: (0, 0, 0))] * 2,
        out_specs=VMEM,
        out_shape=jax.ShapeDtypeStruct((n, seg * width // WIDTH, WIDTH), BF),
        scratch_shapes=[pltpu.VMEM((n * seg, channels), F32)],
        name="out",
    )(core, att, conv, squares, gain[None], own, other)


def sum_kernel(x_ref, out_ref):
    seg = out_ref.shape[0]
    total = x_ref[0].astype(F32)
    for g in range(1, x_ref.shape[0]):
        total = total + x_ref[g].astype(F32)
    for b in range(out_ref.shape[1] // WIDTH):
        block = total[seg * b : seg * b + seg]
        out_ref[:, WIDTH * b : WIDTH * b + WIDTH] = block.astype(BF)


def sum_of(parts, seg):
    return pl.pallas_call(
        sum_kernel,
        in_specs=[VMEM],
        out_specs=VMEM,
        out_shape=jax.ShapeDtypeStruct((seg, parts.shape[1] // seg * WIDTH), BF),
        name="sum",
    )(parts)


def local(
    tokens,
    norm_gain,
    query_weight,
    key_weight,
    value_weight,
    glu_value_weight,
    glu_gate_weight,
    query_gain,
    key_gain,
    lambdas,
    head_gain,
    conv_weight,
    channel_gain,
    attn_out_weight,
    conv_out_weight,
):
    n = lax.axis_size("y")
    heads = query_weight.shape[1] // WIDTH
    tok = tokens.shape[0]
    seg = tok // n
    channels = conv_weight.shape[1]

    row_of = [t // 2 + (n // 2) * (t % 2) for t in range(n)]
    swap = [(y * n + t, row_of[t] * n + y) for y in range(n) for t in range(n)]
    weights = (query_weight, key_weight, value_weight, glu_value_weight, glu_gate_weight)
    weights = weights + (attn_out_weight, conv_out_weight)
    first = sum(w.shape[1] for w in weights[:3])
    columns = sum(w.shape[1] for w in weights)
    shard = lax.ppermute(jnp.concatenate(weights, axis=1), PLANE, swap)
    small = jnp.concatenate(
        [
            conv_weight,
            channel_gain[None],
            jnp.pad(lambdas, (0, channels - heads))[None],
            jnp.zeros((7, channels), F32),
        ],
        axis=0,
    )
    small = lax.ppermute(small, PLANE, swap)
    lambdas = small[CONV_W + 1, :heads]

    blocks = pack(tokens, n)
    mine = lax.all_to_all(blocks, PLANE, 0, 0, tiled=True)
    normed = norm_of(mine, norm_gain, n)

    by_z = lax.all_gather(shard, "z", axis=0)
    core = lax.axis_index("c").astype(jnp.int32)[None]
    mates = [(0, 1), (1, 0)]
    by_z = by_z.reshape(-1, by_z.shape[2])
    wa = copies_to(by_z[:, :first], "x")
    wa_other = lax.ppermute(wa, "c", mates)
    fold = math.log2(math.e) * HEAD_DIM ** (-0.5)
    q_cols = query_weight.shape[1]
    g_cols = glu_value_weight.shape[1]
    late = first + 2 * g_cols
    pad = -(columns - late) % q_cols
    gap = jnp.zeros((by_z.shape[0], pad + q_cols), BF)
    rest = jnp.concatenate([by_z[:, late:], gap, by_z[:, first:late]], axis=1)
    rest = jnp.broadcast_to(rest, (lax.axis_size("x"), *rest.shape))
    rest, kv = qkv(core, normed, wa, wa_other, query_gain * fold, key_gain, rest)
    rest = lax.all_to_all(rest, "x", 0, 0, tiled=True)
    kv = lax.all_gather(kv, "z", axis=0, tiled=True)
    kv_other = lax.ppermute(kv, "c", mates)
    rest_other = lax.ppermute(rest, "c", mates)
    parts = attend(rest, tok, q_cols, kv, kv_other, 1792, 896, 256)
    arrived = lax.all_to_all(parts, "x", 0, 0, tiled=True)
    att = combine(arrived, lambdas, head_gain, tok, heads)

    t = lax.axis_index(TP).astype(jnp.int32)[None]
    glu, heads_rows, tails, edge = glu_of(
        core, t, normed, rest, rest_other, g_cols, n
    )
    size_z = lax.axis_size("z")
    ring = [(i, (i + 1) % n) for i in range(n)]
    left = lax.ppermute(tails, TP, ring)
    right = lax.ppermute(heads_rows, TP, [(b, a) for a, b in ring])
    across = [(z * n + n - 1, (z + 1) * n) for z in range(size_z - 1)]
    across = [(z * n + n - 1, (z + 1) * n) for z in range(size_z - 1)]
    across = across + [(b, a) for a, b in across]
    edge = lax.ppermute(edge, TOK_RING, across)
    conv_sum, squares = conv_of(t, glu, left, right, edge, small[:CONV_W])
    squares = lax.all_to_all(squares, "y", 0, 0, tiled=True)
    term = out_of(
        core, att, conv_sum, squares, small[CONV_W], rest, rest_other, pad
    )
    reduced = lax.all_to_all(term, "y", 0, 0, tiled=True)
    return sum_of(reduced, seg)


def solution(mesh):
    finer = Mesh(mesh.devices.reshape(8, 8, 4, 2), ("z", "y", "x", "c"))
    sp = ("z", "y")
    both, rows = P(sp, TP), P()
    placed = (both, rows) + (both,) * 5 + (rows, rows, P(TP), rows, P(None, TP), P(TP), both, both)
    return jax.shard_map(
        local, mesh=finer, in_specs=placed, out_specs=P(sp + TP, None), check_vma=False
    )
```
